32 devices in a mesh: kv: 8 (over z, y), tp: 4 (over x, core).
Axes of the slice: x: 2, y: 2, z: 4, core: 2. Of those that a mesh axis runs over, the one named last changes fastest.
Arguments:
- tokens: bfloat16 [128, 4096], P('kv'), may hold values from -6 to 6
- dec_tokens: bfloat16 [8, 4096], P('kv'), may hold values from -6 to 6
- norm_gain: float32 [4096], replicated, may hold values from 0.1 to 1.9
- w_query: bfloat16 [2, 4096, 1024], P(None, None, 'tp'), may hold values from -0.09375 to 0.09375
- w_key: bfloat16 [2, 4096, 1024], P(None, None, 'tp'), may hold values from -0.15625 to 0.15625
- w_value: bfloat16 [4096, 2048], P(None, 'tp'), may hold values from -0.09375 to 0.09375
- w_out: bfloat16 [2048, 4096], P('tp'), may hold values from -0.125 to 0.125
- head_gain: float32 [256], replicated, may hold values from 0.1 to 1.9
- mix_lambda: float32 [8], P('tp'), may hold values from 0.3 to 0.8
- ctx_keys: bfloat16 [2, 8192, 1024], P(None, 'kv', 'tp'), may hold values from -600 to 600
- ctx_values: bfloat16 [8192, 2048], P('kv', 'tp'), may hold values from -6 to 6
- dec_keys: bfloat16 [2, 8, 2048, 1024], P(None, 'kv', None, 'tp'), may hold values from -600 to 600
- dec_values: bfloat16 [8, 2048, 2048], P('kv', None, 'tp'), may hold values from -6 to 6
- dec_len: int32 [8], P('kv'), may hold values from 256 to 2048, as said below
Outputs:
- piece_out: bfloat16 [128, 4096], P('kv', 'tp')
- dec_out: bfloat16 [8, 4096], P('kv', 'tp')
The draws below stay inside these ranges and needn't reach their ends.
Inputs may be any that keep to these rules, and one draw needn't show every extreme that they name: `dec_len`: some decoding sequence has exactly 2048 cached positions.
All inputs are finite; a program needn't handle non-finite values.
Results may differ from the reference program's by a relative error of at most 0.03.
The reference program's roundings to bfloat16 on the way count: a program that leaves them out, or rounds other values in their place, can miss the bound.
Values may be sent and summed in bfloat16 or wider, within the bound.
A program may use at most 64 MiB of HBM per device.

```python
import jax
import jax.numpy as jnp
from jax import lax

D = 4096
HEADS = 8
DH = 128
DLEN = 2048
P_SIZE = 128
CTX = 8192
DECS = 8
N_TP = 4


def key_field(key, shape):
    base = jnp.clip(jax.random.normal(key, shape, jnp.float32), -6.0, 6.0) * 1.75
    return base.astype(jnp.bfloat16)


def draw_ctx_keys(key, part):
    return key_field(key, (2, CTX, HEADS * DH))


def draw_dec_keys(key, part):
    return key_field(key, (2, DECS, DLEN, HEADS * DH))


def draw_dec_len(key, part):
    lengths = jax.random.randint(key, (DECS,), DLEN // 8, DLEN + 1)
    chosen = jax.random.randint(jax.random.fold_in(key, 3), (), 0, DECS)
    return jnp.where(jnp.arange(DECS) == chosen, DLEN, lengths).astype(jnp.int32)


def block_scale(stream_key, shape, cuts, smallest, largest):
    def one(axis_at, blocks):
        heights = jax.random.uniform(jax.random.fold_in(jax.random.fold_in(stream_key, 6), axis_at), (blocks,), jnp.float32, smallest / len(cuts), largest / len(cuts))
        return jnp.repeat(jnp.exp(heights), shape[axis_at] // blocks).reshape((-1,) + (1,) * (len(shape) - axis_at - 1))

    loudness = one(*cuts[0])
    for cut in cuts[1:]:
        loudness = loudness * one(*cut)
    return loudness


def bell_draw(key, extent, scale, bound, shards=(), kind=jnp.bfloat16):
    loudness = block_scale(key, extent, shards, -0.22, 0.18) if shards else 1.0
    values = jax.random.normal(key, extent, jnp.float32) * scale * loudness
    return jnp.minimum(jnp.maximum(values, -bound), bound).astype(kind)


def setup_inputs(seed: int = 0) -> dict:
    seeds = jax.random.split(jax.random.key(seed), 15)
    return {
        "tokens": bell_draw(seeds[0], (P_SIZE, D), 1.0, 6.0, ((0, 8),)),
        "dec_tokens": bell_draw(seeds[1], (DECS, D), 1.0, 6.0, ((0, 8),)),
        "norm_gain": jnp.clip(1.0 + 0.18 * jax.random.normal(seeds[2], (D,), jnp.float32), 0.1, 1.9),
        "w_query": bell_draw(seeds[3], (2, D, HEADS * DH), D ** -0.5, 0.09375, ((2, 4),)),
        "w_key": bell_draw(seeds[4], (2, D, HEADS * DH), (D // 3) ** -0.5, 0.15625, ((2, 4),)),
        "w_value": bell_draw(seeds[5], (D, HEADS * 2 * DH), D ** -0.5, 0.09375, ((1, 4),)),
        "w_out": bell_draw(seeds[6], (HEADS * 2 * DH, D), (HEADS * 2 * DH) ** -0.5, 0.125, ((0, 4),)),
        "head_gain": jnp.clip(1.0 + 0.18 * jax.random.normal(seeds[7], (2 * DH,), jnp.float32), 0.1, 1.9),
        "mix_lambda": jnp.clip(0.3 + 0.5 * jax.random.uniform(seeds[8], (HEADS,), jnp.float32) ** block_scale(seeds[8], (HEADS,), ((0, 4),), -0.2, 0.2), 0.3, 0.8),
        "ctx_keys": draw_ctx_keys(jax.random.fold_in(seeds[14], 71), 0),
        "ctx_values": bell_draw(seeds[10], (CTX, HEADS * 2 * DH), 1.0, 6.0, ((0, 8), (1, 4))),
        "dec_keys": draw_dec_keys(jax.random.fold_in(seeds[14], 71), 0),
        "dec_values": bell_draw(seeds[12], (DECS, DLEN, HEADS * 2 * DH), 1.0, 6.0, ((0, 8), (2, 4))),
        "dec_len": draw_dec_len(jax.random.fold_in(seeds[14], 71), 0),
    }


epsilon = 1e-06

def input_rows(rows, norm_gain, w_query, w_key, w_value):
    xf = rows.astype(jnp.float32)
    normed = (xf * lax.rsqrt(lax.optimization_barrier(jnp.mean(xf * xf, axis=-1, keepdims=True)) + epsilon) * norm_gain).astype(jnp.bfloat16)
    query = jnp.stack([jnp.dot(normed, w_query[c], preferred_element_type=jnp.float32) for c in range(2)], 1).astype(jnp.bfloat16)
    keys = jnp.stack([jnp.dot(normed, w_key[c], preferred_element_type=jnp.float32) for c in range(2)], 1).astype(jnp.bfloat16)
    value = jnp.dot(normed, w_value, preferred_element_type=jnp.float32).astype(jnp.bfloat16)
    return (query, keys, value)

def reference(tokens, dec_tokens, norm_gain, w_query, w_key, w_value, w_out, head_gain, mix_lambda, ctx_keys, ctx_values, dec_keys, dec_values, dec_len):
    scale = DH ** (-0.5)
    p_query, p_keys, p_value = input_rows(tokens, norm_gain, w_query, w_key, w_value)
    d_query, d_keys, d_value = input_rows(dec_tokens, norm_gain, w_query, w_key, w_value)
    all_keys = jnp.concatenate([ctx_keys.reshape(2, CTX, HEADS, DH), p_keys.reshape(P_SIZE, 2, HEADS, DH).transpose(1, 0, 2, 3)], axis=1)
    all_keys = all_keys.transpose(2, 0, 1, 3)
    all_values = jnp.concatenate([ctx_values.reshape(CTX, HEADS, 2 * DH), p_value.reshape(P_SIZE, HEADS, 2 * DH)], axis=0)
    all_values = all_values.transpose(1, 0, 2)
    key_pos = jnp.concatenate([jnp.full((CTX,), -1, jnp.int32), jnp.arange(P_SIZE, dtype=jnp.int32)])
    heads_query = p_query.reshape(P_SIZE, 2, HEADS, DH).transpose(2, 1, 0, 3)
    block = 1
    for size in (256, 128, 64, 32, 16, 8, 4, 2, 1):
        if P_SIZE % size == 0 and block == 1:
            block = size
    blocks = P_SIZE // block

    def one_head(args):
        query_h, keys_h, values_h, lam = args
        query_b = query_h.reshape(2, blocks, block, DH).transpose(1, 0, 2, 3)
        pos_b = jnp.arange(P_SIZE, dtype=jnp.int32).reshape(blocks, block)

        def one_block(inner):
            qb, qpos = inner
            valid = key_pos[None, :] <= qpos[:, None]
            probs = []
            for c in range(2):
                scores = jnp.dot(qb[c], keys_h[c].T, preferred_element_type=jnp.float32) * scale
                scores = jnp.where(valid, scores, -jnp.inf)
                top = lax.optimization_barrier(jnp.max(scores, axis=-1, keepdims=True))
                expo = jnp.exp(scores - top)
                probs.append(expo / lax.optimization_barrier(jnp.sum(expo, axis=-1, keepdims=True)))
            weights = (probs[0] - lam * probs[1]).astype(jnp.bfloat16)
            return jnp.dot(weights, values_h, preferred_element_type=jnp.float32)
        return lax.map(one_block, (query_b, pos_b)).reshape(P_SIZE, 2 * DH)
    piece_att = lax.map(one_head, (heads_query, all_keys, all_values, mix_lambda)).transpose(1, 0, 2)

    def one_seq(args):
        query_b, dk_b, dv_b, new_k, new_v, length = args
        keys_b = jnp.concatenate([dk_b.reshape(2, DLEN, HEADS, DH), new_k.reshape(2, 1, HEADS, DH)], axis=1)
        vals_b = jnp.concatenate([dv_b.reshape(DLEN, HEADS, 2 * DH), new_v.reshape(1, HEADS, 2 * DH)], axis=0)
        slot = jnp.arange(DLEN + 1, dtype=jnp.int32)
        valid = (slot < length) | (slot == DLEN)
        probs = []
        for c in range(2):
            scores = jnp.einsum('hd,jhd->hj', query_b[c].reshape(HEADS, DH).astype(jnp.float32), keys_b[c].astype(jnp.float32)) * scale
            scores = jnp.where(valid[None, :], scores, -jnp.inf)
            top = lax.optimization_barrier(jnp.max(scores, axis=-1, keepdims=True))
            expo = jnp.exp(scores - top)
            probs.append(expo / lax.optimization_barrier(jnp.sum(expo, axis=-1, keepdims=True)))
        weights = (probs[0] - mix_lambda[:, None] * probs[1]).astype(jnp.bfloat16)
        return jnp.einsum('hj,jhe->he', weights.astype(jnp.float32), vals_b.astype(jnp.float32))
    dec_keys_seq = dec_keys.transpose(1, 0, 2, 3)
    dec_att = lax.map(one_seq, (d_query, dec_keys_seq, dec_values, d_keys, d_value, dec_len))

    def head_norm(att):
        normed = att * lax.rsqrt(lax.optimization_barrier(jnp.mean(att * att, axis=-1, keepdims=True)) + epsilon) * head_gain
        return normed.astype(jnp.bfloat16).reshape(att.shape[0], HEADS * 2 * DH)

    def project(heads_out):
        group = HEADS // N_TP * 2 * DH
        total = jnp.zeros((heads_out.shape[0], D), jnp.float32)
        for g in range(N_TP):
            part = jnp.dot(heads_out[:, g * group:(g + 1) * group], w_out[g * group:(g + 1) * group], preferred_element_type=jnp.float32)
            part = lax.optimization_barrier(part.astype(jnp.bfloat16))
            total = total + part.astype(jnp.float32)
        return total.astype(jnp.bfloat16)
    return (project(head_norm(piece_att)), project(head_norm(dec_att)))
```

```python
import functools
import math

import jax
import jax.numpy as jnp
from jax import lax
from jax.experimental import pallas as pl
from jax.experimental.pallas import tpu as pltpu
from jax.sharding import PartitionSpec as P

DH = 128
epsilon = 1e-06
MESH = pl.DeviceIdType.MESH
F32 = jnp.float32
BF16 = jnp.bfloat16
LANES = 128
C_EXP = DH ** (-0.5) * math.log2(math.e)
Q_PARTS = 4
K_PARTS = 2
V_PARTS = 4


def dot(a, b):
    return jnp.dot(a, b, preferred_element_type=F32)


def dot_nt(a, b):
    return lax.dot_general(a, b, (((1,), (1,)), ((), ())), preferred_element_type=F32)


def kernel(
    kv, tp,
    tokens, dec_tokens, norm_gain, w_query, w_key, w_value, w_out, head_gain,
    mix_lambda, dec_len, ctx_keys, ctx_values, dec_keys, dec_values,
    out,
    lam_s, len_s, tok_v, dtok_v, gain_v, hgain_v, wq_v, wk_v, wv_v, wo_v,
    ck_v, cv_v, dk_v, dv_v,
    xs, q_all, kown, vown, st_send, st_recv, att_send, att_recv, po_acc, p_send, p_recv,
    d_send, d_recv,
    sem_small, sem_q, sem_k, sem_v, sem_o, sem_c, sem_d,
    qs_sem, qr_sem, ss_sem, sr_sem, as_sem, ar_sem, ps_sem, pr_sem, ds_sem, dr_sem,
):
    me = lax.axis_index("kv")
    mt = lax.axis_index("tp")
    rows, width = tokens.shape
    drows = dec_tokens.shape[0]
    w = w_query.shape[2]
    heads = w // DH
    vw = 2 * DH
    slots = dec_keys.shape[2]
    total = rows * kv
    cols = w_out.shape[1] // tp
    blocks = total // LANES
    padded = xs.shape[0]
    per = LANES // rows

    def tp_peer(d):
        chip = lax.rem(mt // 2 + d // 2, tp // 2)
        return chip * 2 + lax.rem(mt + d, 2)

    barrier = pltpu.get_barrier_semaphore()
    for d in range(1, kv):
        pl.semaphore_signal(
            barrier, inc=1, device_id=(lax.rem(me + d, kv), mt), device_id_type=MESH
        )
    for d in range(1, tp):
        pl.semaphore_signal(
            barrier, inc=1, device_id=(me, tp_peer(d)), device_id_type=MESH
        )

    small = [
        pltpu.make_async_copy(tokens, tok_v, sem_small.at[0]),
        pltpu.make_async_copy(dec_tokens, dtok_v, sem_small.at[1]),
        pltpu.make_async_copy(norm_gain, gain_v, sem_small.at[2]),
        pltpu.make_async_copy(head_gain, hgain_v, sem_small.at[3]),
        pltpu.make_async_copy(mix_lambda, lam_s, sem_small.at[4]),
        pltpu.make_async_copy(dec_len, len_s, sem_small.at[5]),
    ]
    for c in small:
        c.start()

    qstep = width // Q_PARTS
    kstep = width // K_PARTS
    vstep = width // V_PARTS
    q_copies = []
    for h in range(heads):
        q_copies.append([])
        for i in range(Q_PARTS):
            sl = (slice(None), pl.ds(i * qstep, qstep), pl.ds(h * DH, DH))
            q_copies[h].append(
                pltpu.make_async_copy(
                    w_query.at[sl], wq_v.at[sl], sem_q.at[h * Q_PARTS + i]
                )
            )
    k_copies = []
    for i in range(K_PARTS):
        sl = (slice(None), pl.ds(i * kstep, kstep))
        k_copies.append(pltpu.make_async_copy(w_key.at[sl], wk_v.at[sl], sem_k.at[i]))
    v_copies = [
        pltpu.make_async_copy(
            w_value.at[pl.ds(i * vstep, vstep)], wv_v.at[pl.ds(i * vstep, vstep)], sem_v.at[i]
        )
        for i in range(V_PARTS)
    ]
    ck_copy = pltpu.make_async_copy(ctx_keys, ck_v, sem_c.at[0])
    cv_copy = pltpu.make_async_copy(ctx_values, cv_v, sem_c.at[1])
    dk_copy = pltpu.make_async_copy(dec_keys, dk_v, sem_d.at[0])
    dv_copy = pltpu.make_async_copy(dec_values, dv_v, sem_d.at[1])
    wo_copies = []
    for d in range(tp):
        start = pl.multiple_of(tp_peer(d) * cols, LANES)
        wo_copies.append(
            pltpu.make_async_copy(w_out.at[:, pl.ds(start, cols)], wo_v.at[d], sem_o.at[d])
        )
    for row in q_copies:
        for c in row:
            c.start()

    kown[...] = jnp.zeros_like(kown)
    vown[...] = jnp.zeros_like(vown)
    xs[rows:, :] = jnp.zeros((padded - rows, width), BF16)
    for c in small:
        c.wait()
    gain = gain_v[...]

    def normed(x):
        xf = x.astype(F32)
        inv = lax.rsqrt(jnp.mean(xf * xf, axis=-1, keepdims=True) + epsilon)
        return (xf * inv * gain).astype(BF16)

    xs[0:rows, :] = normed(tok_v[...])
    xs[rows : rows + drows, :] = normed(dtok_v[...])

    def to_kv(src, dst, send, recv, d):
        return pltpu.make_async_remote_copy(
            src_ref=src, dst_ref=dst, send_sem=send, recv_sem=recv,
            device_id=(lax.rem(me + d, kv), mt), device_id_type=MESH,
        )

    far_first = sorted(range(1, kv), key=lambda d: (-min(d, kv - d), d))
    dec_qh = []
    q_sends = []
    for h in range(heads):
        hs = slice(h * DH, (h + 1) * DH)
        acc = None
        for i in range(Q_PARTS):
            q_copies[h][i].wait()
            sl = slice(i * qstep, (i + 1) * qstep)
            wt = jnp.concatenate([wq_v[0, sl, hs], wq_v[1, sl, hs]], axis=1)
            term = dot(xs[:, sl], wt)
            acc = term if acc is None else acc + term
        qh = acc.astype(BF16)
        q_all[h, me] = qh[0:rows]
        dec_qh.append(qh[rows:])
        if h == 0:
            for c in k_copies + [ck_copy]:
                c.start()
        if h == heads - 1:
            for c in v_copies + [cv_copy]:
                c.start()
        if h == 0:
            pl.semaphore_wait(barrier, kv + tp - 2)
        q_sends.append(
            {
                d: to_kv(q_all.at[h, me], q_all.at[h, me], qs_sem.at[h, d], qr_sem.at[h, d], d)
                for d in far_first
            }
        )
        for d in far_first:
            q_sends[h][d].start()

    acc = [None, None]
    for i in range(K_PARTS):
        k_copies[i].wait()
        sl = slice(i * kstep, (i + 1) * kstep)
        for c in range(2):
            term = dot(xs[:, sl], wk_v[c, sl, :])
            acc[c] = term if acc[c] is None else acc[c] + term
    dec_k = []
    for c in range(2):
        kc = acc[c].astype(BF16)
        kown[c, 0:rows, :] = kc[0:rows]
        dec_k.append(kc[rows:])
    for c in [dk_copy, dv_copy]:
        c.start()
    acc = None
    for i in range(V_PARTS):
        v_copies[i].wait()
        term = dot(xs[:, i * vstep : (i + 1) * vstep], wv_v[i * vstep : (i + 1) * vstep, :])
        acc = term if acc is None else acc + term
    vc = acc.astype(BF16)
    vown[0:rows, :] = vc[0:rows]
    dec_v = vc[rows:]
    for c in wo_copies:
        c.start()

    ck_copy.wait()
    cv_copy.wait()
    nstat = 4

    def head_block(h, b):
        slots_b = pl.ds(b * per, per)
        qb = q_all[h, slots_b].reshape(LANES, 2 * DH)
        pos = b * LANES + lax.broadcasted_iota(jnp.int32, (LANES, LANES), 0)
        lane = lax.broadcasted_iota(jnp.int32, (LANES, LANES), 1)
        ok = (lane < rows) & (lane + me * rows <= pos)
        stats = jnp.zeros((LANES, LANES), F32)
        hs = slice(h * DH, (h + 1) * DH)
        hv = slice(h * vw, (h + 1) * vw)
        far_p = []
        near_p = []
        for c in range(2):
            q = qb[:, c * DH : (c + 1) * DH]
            far = dot_nt(q, ck_v[c, :, hs])
            near = dot_nt(q, kown[c, :, hs])
            near = jnp.where(ok, near, -jnp.inf)
            top = jnp.maximum(
                jnp.max(far, axis=-1, keepdims=True), jnp.max(near, axis=-1, keepdims=True)
            )
            ef = jnp.exp2((far - top) * C_EXP)
            en = jnp.exp2((near - top) * C_EXP)
            tot = jnp.sum(ef, axis=-1, keepdims=True) + jnp.sum(en, axis=-1, keepdims=True)
            far_p.append(ef.astype(BF16))
            near_p.append(en.astype(BF16))
            stats = jnp.where(lane == c, top, stats)
            stats = jnp.where(lane == 2 + c, tot, stats)
        for c in range(2):
            att = dot(far_p[c], cv_v[:, hv]) + dot(near_p[c], vown[:, hv])
            att_send[h, slots_b, :, c * vw : (c + 1) * vw] = att.astype(BF16).reshape(
                per, rows, vw
            )
        by_row = jnp.transpose(stats)
        lane8 = lax.broadcasted_iota(jnp.int32, (per, LANES), 1) // rows
        packed = jnp.zeros((per, LANES), F32)
        for s in range(nstat):
            line = jnp.broadcast_to(by_row[s : s + 1, :], (per, LANES))
            line = pltpu.roll(line, rows, 1, stride=rows, stride_axis=0)
            if s:
                line = pltpu.roll(line, s * rows, 1)
            packed = jnp.where(lane8 == s, line, packed)
        for o in range(per):
            st_send[h, b * per + o] = packed[per - 1 - o : per - o, :]

    a_sends = []
    st_sends = []
    for h in range(heads):
        for d in far_first:
            q_sends[h][d].wait_recv()
        if blocks == 1:
            head_block(h, 0)
        else:
            pl.loop(0, blocks)(functools.partial(head_block, h))
        st_recv[h, 0] = st_send[h, me]
        for i in range(kv - 1):
            peer = i + jnp.where(me <= i, 1, 0)
            d = lax.rem(peer - me + kv, kv)
            to_kv(
                st_send.at[h, peer], st_recv.at[h, d], ss_sem.at[h, d], sr_sem.at[h, d], d
            ).start()
        for i in range(kv - 1):
            peer = i + jnp.where(me <= i, 1, 0)
            d = lax.rem(peer - me + kv, kv)
            to_kv(
                att_send.at[h, peer], att_recv.at[h, d], as_sem.at[h, d], ar_sem.at[h, d], d
            ).start()
        st_sends.append({})
        a_sends.append({})
        for d in range(1, kv):
            peer = lax.rem(me + d, kv)
            st_sends[h][d] = to_kv(
                st_send.at[h, peer], st_recv.at[h, d], ss_sem.at[h, d], sr_sem.at[h, d], d
            )
            a_sends[h][d] = to_kv(
                att_send.at[h, peer], att_recv.at[h, d], as_sem.at[h, d], ar_sem.at[h, d], d
            )

    hgain = hgain_v[...]
    group = 16
    hrow = lax.broadcasted_iota(jnp.int32, (group, w), 0)
    hcol = lax.broadcasted_iota(jnp.int32, (group, w), 1) // DH
    own_head = hrow == hcol
    row1 = lax.broadcasted_iota(jnp.int32, (group, 1), 0)
    lam_col = jnp.zeros((group, 1), F32)
    for h in range(heads):
        lam_col = jnp.where(row1 == h, lam_s[h], lam_col)
    dk_copy.wait()
    slot_id = lax.broadcasted_iota(jnp.int32, (group, slots), 1)
    vrow = lax.broadcasted_iota(jnp.int32, (group, heads * vw), 0)
    vcol = lax.broadcasted_iota(jnp.int32, (group, heads * vw), 1) // vw
    dec_q = [
        jnp.concatenate([q[:, c * DH : (c + 1) * DH] for q in dec_qh], axis=1) for c in range(2)
    ]
    dec_att = []
    for r in range(drows):
        far_p = []
        near_p = []
        for c in range(2):
            qr = jnp.broadcast_to(dec_q[c][r : r + 1].astype(F32), (group, w))
            qr = jnp.where(own_head, qr, 0.0)
            kr = dec_k[c][r : r + 1].astype(F32)
            near = jnp.sum(qr * kr, axis=-1, keepdims=True)
            far = dot_nt(qr.astype(BF16), dk_v[c, r])
            far = jnp.where(slot_id < len_s[r], far, -jnp.inf)
            top = jnp.maximum(jnp.max(far, axis=-1, keepdims=True), near)
            ef = jnp.exp2((far - top) * C_EXP)
            en = jnp.exp2((near - top) * C_EXP)
            den = jnp.sum(ef, axis=-1, keepdims=True) + en
            far_p.append(ef / den)
            near_p.append(en / den)
        far_w = (far_p[0] - lam_col * far_p[1]).astype(BF16)
        near_w = (near_p[0] - lam_col * near_p[1]).astype(BF16).astype(F32)
        if r == 0:
            dv_copy.wait()
        att = dot(far_w, dv_v[r]) + near_w * dec_v[r : r + 1].astype(F32)
        dec_att.append(jnp.sum(jnp.where(vrow == vcol, att, 0.0), axis=0, keepdims=True))

    def head_norm(att):
        inv = lax.rsqrt(jnp.mean(att * att, axis=-1, keepdims=True) + epsilon)
        return (att * inv * hgain).astype(BF16)

    def to_tp(src, dst, send, recv, d):
        return pltpu.make_async_remote_copy(
            src_ref=src.at[d], dst_ref=dst.at[d], send_sem=send.at[d], recv_sem=recv.at[d],
            device_id=(me, tp_peer(d)), device_id_type=MESH,
        )

    def out_part(ho, d, h):
        return dot(ho, wo_v[d, h * vw : (h + 1) * vw, :])

    dec_rows = jnp.concatenate(dec_att, axis=0) if drows > 1 else dec_att[0]
    dec_rows = dec_rows if drows > 1 else jnp.broadcast_to(dec_rows, (group, heads * vw))
    dec_ho = [head_norm(dec_rows[:, h * vw : (h + 1) * vw]) for h in range(heads)]
    for c in wo_copies:
        c.wait()
    order = list(range(tp - 1, 0, -1))

    def dec_project(d):
        acc = None
        for h in range(heads):
            term = out_part(dec_ho[h], d, h)
            acc = term if acc is None else acc + term
        return acc[0:drows].astype(BF16)

    d_sends = {d: to_tp(d_send, d_recv, ds_sem, dr_sem, d) for d in order}
    for d in order:
        d_send[d] = dec_project(d)
        d_sends[d].start()
    dec_own = dec_project(0)

    lane = lax.broadcasted_iota(jnp.int32, (1, LANES), 1)
    p_sends = {d: to_tp(p_send, p_recv, ps_sem, pr_sem, d) for d in order}
    own = None
    for h in range(heads):
        for d in range(1, kv):
            st_sends[h][d].wait_recv()
        sts = st_recv[h].reshape(kv, LANES)
        top = jnp.max(sts, axis=0, keepdims=True)
        fac = jnp.exp2((sts - top) * C_EXP)
        den = jnp.sum(fac * pltpu.roll(sts, LANES - 2 * rows, 1), axis=0, keepdims=True)
        den = jnp.where(lane < 2 * rows, den, 1.0)
        part = jnp.where(lane < rows, 1.0, -lam_s[h]) / den
        fac = jnp.transpose(fac * part)
        total_att = None
        for d in [0] + far_first[::-1]:
            if d == 0:
                blk = att_send[h, me]
            else:
                a_sends[h][d].wait_recv()
                blk = att_recv[h, d]
            for c in range(2):
                term = fac[c * rows : (c + 1) * rows, d : d + 1] * blk[
                    :, c * vw : (c + 1) * vw
                ].astype(F32)
                total_att = term if total_att is None else total_att + term
        ho = head_norm(total_att)
        last = h == heads - 1
        for d in order + [0]:
            term = out_part(ho, d, h)
            if h > 0:
                term = term + po_acc[d]
            if not last:
                po_acc[d] = term
            elif d > 0:
                p_send[d] = term.astype(BF16)
                p_sends[d].start()
            else:
                own = term.astype(BF16).astype(F32)
    dsum = dec_own.astype(F32)
    for d in order:
        d_sends[d].wait_recv()
        dsum = dsum + d_recv[d].astype(F32)
    out[rows:, :] = jnp.broadcast_to(dsum, (out.shape[0] - rows, cols)).astype(BF16) if (
        drows == 1
    ) else jnp.concatenate(
        [dsum, jnp.zeros((out.shape[0] - rows - drows, cols), F32)], axis=0
    ).astype(BF16)
    for rem_sends in q_sends + st_sends + a_sends:
        for d in range(1, kv):
            rem_sends[d].wait_send()
    for d in order:
        d_sends[d].wait_send()
    for d in order[::-1]:
        p_sends[d].wait_recv()
        own = own + p_recv[d].astype(F32)
    out[0:rows, :] = own.astype(BF16)
    for d in order:
        p_sends[d].wait_send()


def body(
    tokens, dec_tokens, norm_gain, w_query, w_key, w_value, w_out, head_gain, mix_lambda,
    ctx_keys, ctx_values, dec_keys, dec_values, dec_len, *, kv, tp,
):
    rows, width = tokens.shape
    drows = dec_tokens.shape[0]
    w = w_query.shape[2]
    heads = w // DH
    vwid = w_value.shape[1]
    ctx = ctx_keys.shape[1]
    slots = dec_keys.shape[2]
    cols = w_out.shape[1] // tp
    padded = rows + -(-drows // 16) * 16
    any_spec = pl.BlockSpec(memory_space=pltpu.HBM)
    vmem = pl.BlockSpec(memory_space=pltpu.VMEM)
    dma = pltpu.SemaphoreType.DMA
    V = pltpu.VMEM

    def hbm(x):
        return pltpu.with_memory_space_constraint(x, pltpu.HBM) if x.size > 1 else x

    out = pl.pallas_call(
        functools.partial(kernel, kv, tp),
        out_shape=jax.ShapeDtypeStruct((padded, cols), BF16),
        in_specs=[any_spec] * 8 + [pl.BlockSpec(memory_space=pl.ANY)] * 2 + [any_spec] * 4,
        out_specs=vmem,
        scratch_shapes=[
            pltpu.SMEM((heads,), F32), pltpu.SMEM((drows,), jnp.int32),
            V((rows, width), BF16), V((drows, width), BF16), V((1, width), F32),
            V((1, 2 * DH), F32),
            V((2, width, w), BF16), V((2, width, w), BF16), V((width, vwid), BF16),
            V((tp, vwid, cols), BF16),
            V((2, ctx, w), BF16), V((ctx, vwid), BF16),
            V((2, drows, slots, w), BF16), V((drows, slots, vwid), BF16),
            V((padded, width), BF16), V((heads, kv, rows, 2 * DH), BF16),
            V((2, LANES, w), BF16), V((LANES, vwid), BF16),
            V((heads, kv, 1, LANES), F32), V((heads, kv, 1, LANES), F32),
            V((heads, kv, rows, 4 * DH), BF16), V((heads, kv, rows, 4 * DH), BF16),
            V((tp, rows, cols), F32),
            V((tp, rows, cols), BF16), V((tp, rows, cols), BF16),
            V((tp, drows, cols), BF16), V((tp, drows, cols), BF16),
            dma((6,)), dma((heads * Q_PARTS,)), dma((K_PARTS,)), dma((V_PARTS,)), dma((tp,)),
            dma((2,)), dma((2,)),
            dma((heads, kv)), dma((heads, kv)), dma((heads, kv)), dma((heads, kv)),
            dma((heads, kv)), dma((heads, kv)),
            dma((tp,)), dma((tp,)), dma((tp,)), dma((tp,)),
        ],
        compiler_params=pltpu.CompilerParams(
            collective_id=0, has_side_effects=True, vmem_limit_bytes=48 * 1024 * 1024
        ),
    )(
        hbm(tokens), hbm(dec_tokens), hbm(norm_gain.reshape(1, width)), hbm(w_query),
        hbm(w_key), hbm(w_value), hbm(w_out), hbm(head_gain.reshape(1, 2 * DH)),
        hbm(mix_lambda), hbm(dec_len), hbm(ctx_keys), hbm(ctx_values), hbm(dec_keys),
        hbm(dec_values),
    )

    def split(src, piece_ref, dec_ref):
        piece_ref[...] = src[0:rows, :]
        dec_ref[...] = src[rows : rows + drows, :]

    return pl.pallas_call(
        split,
        out_shape=(
            jax.ShapeDtypeStruct((rows, cols), BF16),
            jax.ShapeDtypeStruct((drows, cols), BF16),
        ),
        in_specs=[vmem],
        out_specs=(vmem, vmem),
        compiler_params=pltpu.CompilerParams(vmem_limit_bytes=1024 * 1024),
    )(out)


def solution(mesh):
    in_specs = (
        P("kv", None),
        P("kv", None),
        P(),
        P(None, None, "tp"),
        P(None, None, "tp"),
        P(None, "tp"),
        P("tp", None),
        P(),
        P("tp"),
        P(None, "kv", "tp"),
        P("kv", "tp"),
        P(None, "kv", None, "tp"),
        P("kv", None, "tp"),
        P("kv"),
    )
    out_specs = (P("kv", "tp"), P("kv", "tp"))
    step = functools.partial(body, kv=mesh.shape["kv"], tp=mesh.shape["tp"])
    return jax.shard_map(step, mesh=mesh, in_specs=in_specs, out_specs=out_specs, check_vma=False)
```

```python
import functools
import math

import jax
import jax.numpy as jnp
from jax import lax
from jax.experimental import pallas as pl
from jax.experimental.pallas import tpu as pltpu
from jax.sharding import PartitionSpec as P

DH = 128
epsilon = 1e-06
MESH = pl.DeviceIdType.MESH
F32 = jnp.float32
BF16 = jnp.bfloat16
LANES = 128
C_EXP = DH ** (-0.5) * math.log2(math.e)
Q_PARTS = 8
K_PARTS = 2
BLOCK = 64
UNROLL = 4
V_PARTS = 4


def dot(a, b):
    return jnp.dot(a, b, preferred_element_type=F32)


def dot_nt(a, b):
    return lax.dot_general(a, b, (((1,), (1,)), ((), ())), preferred_element_type=F32)


def piece_block(total):
    return BLOCK if total % BLOCK == 0 else LANES


def kernel(
    kv, tp,
    tokens, dec_tokens, norm_gain, w_query, w_key, w_value, w_out, head_gain,
    mix_lambda, dec_len, ctx_keys, ctx_values, dec_keys, dec_values,
    out,
    lam_s, len_s, tok_v, dtok_v, gain_v, hgain_v, wq_v, wk_v, wv_v, wo_v,
    ck_v, cv_v, dk_v, dv_v,
    xs, q_all, kown, vown, st_send, st_recv, fac_v, att_send, att_recv, po_acc, p_send, p_recv,
    d_send, d_recv,
    sem_small, sem_q, sem_k, sem_v, sem_o, sem_c, sem_d,
    qs_sem, qr_sem, ss_sem, sr_sem, as_sem, ar_sem, ps_sem, pr_sem, ds_sem, dr_sem,
):
    me = lax.axis_index("kv")
    mt = lax.axis_index("tp")
    rows, width = tokens.shape
    drows = dec_tokens.shape[0]
    w = w_query.shape[2]
    heads = w // DH
    vw = 2 * DH
    slots = dec_keys.shape[2]
    total = rows * kv
    cols = w_out.shape[1] // tp
    block = piece_block(total)
    blocks = total // block
    padded = xs.shape[0]
    per = block // rows

    def tp_peer(d):
        chip = lax.rem(mt // 2 + d // 2, tp // 2)
        return chip * 2 + lax.rem(mt + d, 2)

    barrier = pltpu.get_barrier_semaphore()
    for d in range(1, kv):
        pl.semaphore_signal(
            barrier, inc=1, device_id=(lax.rem(me + d, kv), mt), device_id_type=MESH
        )
    for d in range(1, tp):
        pl.semaphore_signal(
            barrier, inc=1, device_id=(me, tp_peer(d)), device_id_type=MESH
        )

    small = [
        pltpu.make_async_copy(tokens, tok_v, sem_small.at[0]),
        pltpu.make_async_copy(dec_tokens, dtok_v, sem_small.at[1]),
        pltpu.make_async_copy(norm_gain, gain_v, sem_small.at[2]),
        pltpu.make_async_copy(head_gain, hgain_v, sem_small.at[3]),
        pltpu.make_async_copy(mix_lambda, lam_s, sem_small.at[4]),
        pltpu.make_async_copy(dec_len, len_s, sem_small.at[5]),
    ]
    for c in small:
        c.start()

    qstep = width // Q_PARTS
    kstep = width // K_PARTS
    vstep = width // V_PARTS
    q_copies = []
    for i in range(Q_PARTS):
        sl = (slice(None), pl.ds(i * qstep, qstep))
        q_copies.append(pltpu.make_async_copy(w_query.at[sl], wq_v.at[sl], sem_q.at[i]))
    k_copies = []
    for i in range(K_PARTS):
        sl = (slice(None), pl.ds(i * kstep, kstep))
        k_copies.append(pltpu.make_async_copy(w_key.at[sl], wk_v.at[sl], sem_k.at[i]))
    v_copies = [
        pltpu.make_async_copy(
            w_value.at[pl.ds(i * vstep, vstep)], wv_v.at[pl.ds(i * vstep, vstep)], sem_v.at[i]
        )
        for i in range(V_PARTS)
    ]
    ck_copy = pltpu.make_async_copy(ctx_keys, ck_v, sem_c.at[0])
    cv_copy = pltpu.make_async_copy(ctx_values, cv_v, sem_c.at[1])
    dk_copy = pltpu.make_async_copy(dec_keys, dk_v, sem_d.at[0])
    dv_copy = pltpu.make_async_copy(dec_values, dv_v, sem_d.at[1])
    wo_copies = []
    for d in range(tp):
        start = pl.multiple_of(tp_peer(d) * cols, LANES)
        wo_copies.append(
            pltpu.make_async_copy(w_out.at[:, pl.ds(start, cols)], wo_v.at[d], sem_o.at[d])
        )
    for c in q_copies:
        c.start()

    kown[...] = jnp.zeros_like(kown)
    vown[...] = jnp.zeros_like(vown)
    xs[rows:, :] = jnp.zeros((padded - rows, width), BF16)
    for c in small:
        c.wait()
    gain = gain_v[...]

    def normed(x):
        xf = x.astype(F32)
        inv = lax.rsqrt(jnp.mean(xf * xf, axis=-1, keepdims=True) + epsilon)
        return (xf * inv * gain).astype(BF16)

    xs[0:rows, :] = normed(tok_v[...])
    xs[rows : rows + drows, :] = normed(dtok_v[...])

    def to_kv(src, dst, send, recv, d):
        return pltpu.make_async_remote_copy(
            src_ref=src, dst_ref=dst, send_sem=send, recv_sem=recv,
            device_id=(lax.rem(me + d, kv), mt), device_id_type=MESH,
        )

    def drain(ref, sem):
        pltpu.make_async_copy(ref, ref, sem).wait()

    far_first = sorted(range(1, kv), key=lambda d: (-min(d, kv - d), d))
    for c in k_copies + [ck_copy]:
        c.start()
    acc = [None, None]
    for i in range(Q_PARTS):
        q_copies[i].wait()
        sl = slice(i * qstep, (i + 1) * qstep)
        for c in range(2):
            term = dot(xs[:, sl], wq_v[c, sl, :])
            acc[c] = term if acc[c] is None else acc[c] + term
    dec_q = []
    for c in range(2):
        qc = acc[c].astype(BF16)
        q_all[me, :, c * w : (c + 1) * w] = qc[0:rows]
        dec_q.append(qc[rows:])
    for c in v_copies + [cv_copy]:
        c.start()
    pl.semaphore_wait(barrier, kv + tp - 2)
    for d in far_first:
        to_kv(q_all.at[me], q_all.at[me], qs_sem, qr_sem.at[lax.div(me, per)], d).start()

    acc = [None, None]
    for i in range(K_PARTS):
        k_copies[i].wait()
        sl = slice(i * kstep, (i + 1) * kstep)
        for c in range(2):
            term = dot(xs[:, sl], wk_v[c, sl, :])
            acc[c] = term if acc[c] is None else acc[c] + term
    dec_k = []
    for c in range(2):
        kc = acc[c].astype(BF16)
        kown[c, 0:rows, :] = kc[0:rows]
        dec_k.append(kc[rows:])
    for c in [dk_copy, dv_copy]:
        c.start()
    acc = None
    for i in range(V_PARTS):
        v_copies[i].wait()
        term = dot(xs[:, i * vstep : (i + 1) * vstep], wv_v[i * vstep : (i + 1) * vstep, :])
        acc = term if acc is None else acc + term
    vc = acc.astype(BF16)
    vown[0:rows, :] = vc[0:rows]
    dec_v = vc[rows:]
    for c in wo_copies:
        c.start()

    ck_copy.wait()
    cv_copy.wait()
    nstat = 4 * heads
    most = LANES // rows

    def wait_queries(b):
        inside = lax.div(me, per) == b

        @pl.when(inside)
        def _():
            drain(q_all.at[pl.ds(b * per, per - 1)], qr_sem.at[b])

        @pl.when(jnp.logical_not(inside))
        def _():
            drain(q_all.at[pl.ds(b * per, per)], qr_sem.at[b])

    def attend(b):
        slots_b = pl.ds(b * per, per)
        qb = q_all[slots_b].reshape(block, 2 * w)
        pos = b * block + lax.broadcasted_iota(jnp.int32, (block, LANES), 0)
        lane = lax.broadcasted_iota(jnp.int32, (block, LANES), 1)
        ok = (lane < rows) & (lane + me * rows <= pos)
        ok = jnp.concatenate([ok] * heads, axis=0) if heads > 1 else ok
        head_of = lax.broadcasted_iota(jnp.int32, (block, w), 1) // DH
        stats = jnp.zeros((block, LANES), F32)
        far_p = []
        near_p = []
        for c in range(2):
            qc = qb[:, c * w : (c + 1) * w]
            if heads > 1:
                zero = jnp.zeros_like(qc)
                qc = jnp.concatenate(
                    [jnp.where(head_of == h, qc, zero) for h in range(heads)], axis=0
                )
            far = dot_nt(qc, ck_v[c])
            near = dot_nt(qc, kown[c])
            near = jnp.where(ok, near, -jnp.inf)
            top = jnp.maximum(
                jnp.max(far, axis=-1, keepdims=True), jnp.max(near, axis=-1, keepdims=True)
            )
            ef = jnp.exp2((far - top) * C_EXP)
            en = jnp.exp2((near - top) * C_EXP)
            tot = jnp.sum(ef, axis=-1, keepdims=True) + jnp.sum(en, axis=-1, keepdims=True)
            far_p.append(ef.astype(BF16))
            near_p.append(en.astype(BF16))
            for h in range(heads):
                part = slice(h * block, (h + 1) * block)
                stats = jnp.where(lane == 2 * h + c, top[part], stats)
                stats = jnp.where(lane == 2 * heads + 2 * h + c, tot[part], stats)
        for h in range(heads):
            part = slice(h * block, (h + 1) * block)
            hv = slice(h * vw, (h + 1) * vw)
            att = dot(jnp.concatenate([p[part] for p in far_p], axis=0), cv_v[:, hv]) + dot(
                jnp.concatenate([p[part] for p in near_p], axis=0), vown[:, hv]
            )
            for c in range(2):
                att_send[h, slots_b, :, c * vw : (c + 1) * vw] = (
                    att[c * block : (c + 1) * block].astype(BF16).reshape(per, rows, vw)
                )
        if block < LANES:
            stats = jnp.concatenate([stats, jnp.zeros((LANES - block, LANES), F32)], axis=0)
        by_row = jnp.transpose(stats)
        group_of = lax.broadcasted_iota(jnp.int32, (most, LANES), 1) // rows
        packed = jnp.zeros((most, LANES), F32)
        for s in range(nstat):
            line = jnp.broadcast_to(by_row[s : s + 1, :], (most, LANES))
            line = pltpu.roll(line, rows, 1, stride=rows, stride_axis=0)
            if s:
                line = pltpu.roll(line, s * rows, 1)
            packed = jnp.where(group_of == s, line, packed)
        for o in range(per):
            st_send[b * per + o] = packed[most - 1 - o : most - o, :]

    def send_block(peers):
        for peer in peers:
            d = lax.rem(peer - me + kv, kv)

            @pl.when(peer != me)
            def _(peer=peer, d=d):
                to_kv(st_send.at[peer], st_recv.at[d], ss_sem, sr_sem, d).start()

        for peer in peers:
            d = lax.rem(peer - me + kv, kv)

            @pl.when(peer != me)
            def _(peer=peer, d=d):
                for h in range(heads):
                    to_kv(
                        att_send.at[h, peer], att_recv.at[h, d], as_sem, ar_sem.at[h], d
                    ).start()

    if blocks <= UNROLL:
        for b in range(blocks):
            wait_queries(b)
            attend(b)
            send_block(range(b * per, (b + 1) * per))
    else:
        for b in range(blocks):
            wait_queries(b)
        pl.loop(0, blocks)(attend)
        send_block(range(kv))
    st_recv[0] = st_send[me]

    hgain = hgain_v[...]
    group = 16
    hrow = lax.broadcasted_iota(jnp.int32, (group, w), 0)
    hcol = lax.broadcasted_iota(jnp.int32, (group, w), 1) // DH
    own_head = hrow == hcol
    row1 = lax.broadcasted_iota(jnp.int32, (group, 1), 0)
    lam_col = jnp.zeros((group, 1), F32)
    for h in range(heads):
        lam_col = jnp.where(row1 == h, lam_s[h], lam_col)
    dk_copy.wait()
    slot_id = lax.broadcasted_iota(jnp.int32, (group, slots), 1)
    vrow = lax.broadcasted_iota(jnp.int32, (group, heads * vw), 0)
    vcol = lax.broadcasted_iota(jnp.int32, (group, heads * vw), 1) // vw
    dec_att = []
    for r in range(drows):
        far_p = []
        near_p = []
        for c in range(2):
            qr = jnp.broadcast_to(dec_q[c][r : r + 1].astype(F32), (group, w))
            qr = jnp.where(own_head, qr, 0.0)
            kr = dec_k[c][r : r + 1].astype(F32)
            near = jnp.sum(qr * kr, axis=-1, keepdims=True)
            far = dot_nt(qr.astype(BF16), dk_v[c, r])
            far = jnp.where(slot_id < len_s[r], far, -jnp.inf)
            top = jnp.maximum(jnp.max(far, axis=-1, keepdims=True), near)
            ef = jnp.exp2((far - top) * C_EXP)
            en = jnp.exp2((near - top) * C_EXP)
            den = jnp.sum(ef, axis=-1, keepdims=True) + en
            far_p.append(ef / den)
            near_p.append(en / den)
        far_w = (far_p[0] - lam_col * far_p[1]).astype(BF16)
        near_w = (near_p[0] - lam_col * near_p[1]).astype(BF16).astype(F32)
        if r == 0:
            dv_copy.wait()
        att = dot(far_w, dv_v[r]) + near_w * dec_v[r : r + 1].astype(F32)
        dec_att.append(jnp.sum(jnp.where(vrow == vcol, att, 0.0), axis=0, keepdims=True))

    def head_norm(att):
        inv = lax.rsqrt(jnp.mean(att * att, axis=-1, keepdims=True) + epsilon)
        return (att * inv * hgain).astype(BF16)

    def to_tp(src, dst, send, recv, d):
        return pltpu.make_async_remote_copy(
            src_ref=src.at[d], dst_ref=dst.at[d], send_sem=send, recv_sem=recv,
            device_id=(me, tp_peer(d)), device_id_type=MESH,
        )

    def out_part(ho, d, h):
        return dot(ho, wo_v[d, h * vw : (h + 1) * vw, :])

    dec_rows = jnp.concatenate(dec_att, axis=0) if drows > 1 else dec_att[0]
    dec_rows = dec_rows if drows > 1 else jnp.broadcast_to(dec_rows, (group, heads * vw))
    dec_ho = [head_norm(dec_rows[:, h * vw : (h + 1) * vw]) for h in range(heads)]
    for c in wo_copies:
        c.wait()
    order = list(range(tp - 1, 0, -1))

    def dec_project(d):
        acc = None
        for h in range(heads):
            term = out_part(dec_ho[h], d, h)
            acc = term if acc is None else acc + term
        return acc[0:drows].astype(BF16)

    d_sends = {d: to_tp(d_send, d_recv, ds_sem, dr_sem, d) for d in order}
    for d in order:
        d_send[d] = dec_project(d)
        d_sends[d].start()
    dec_own = dec_project(0)

    lane = lax.broadcasted_iota(jnp.int32, (1, LANES), 1)
    p_sends = {d: to_tp(p_send, p_recv, ps_sem, pr_sem, d) for d in order}
    drain(st_recv.at[pl.ds(1, kv - 1)], sr_sem)
    nmax = 2 * heads * rows
    sts = st_recv[...].reshape(kv, LANES)
    top = jnp.max(sts, axis=0, keepdims=True)
    fac = jnp.exp2((sts - top) * C_EXP)
    den = jnp.sum(fac * pltpu.roll(sts, LANES - nmax, 1), axis=0, keepdims=True)
    den = jnp.where(lane < nmax, den, 1.0)
    sign = jnp.ones((1, LANES), F32)
    for h in range(heads):
        sign = jnp.where(lane // rows == 2 * h + 1, -lam_s[h], sign)
    fac = jnp.transpose(fac * (sign / den))
    for i in range(2 * heads):
        for d in range(kv):
            fac_v[i, d] = jnp.broadcast_to(
                fac[i * rows : (i + 1) * rows, d : d + 1], (rows, LANES)
            )
    own = None
    for h in range(heads):
        drain(att_recv.at[h, pl.ds(1, kv - 1)], ar_sem.at[h])
        total_att = None
        for d in range(kv):
            blk = att_send[h, me] if d == 0 else att_recv[h, d]
            for c in range(2):
                f = fac_v[2 * h + c, d]
                term = jnp.concatenate([f] * (vw // LANES), axis=1) * blk[
                    :, c * vw : (c + 1) * vw
                ].astype(F32)
                total_att = term if total_att is None else total_att + term
        ho = head_norm(total_att)
        last = h == heads - 1
        for d in order + [0]:
            term = out_part(ho, d, h)
            if h > 0:
                term = term + po_acc[d]
            if not last:
                po_acc[d] = term
            elif d > 0:
                p_send[d] = term.astype(BF16)
            else:
                own = term.astype(BF16).astype(F32)
        if last:
            for d in order:
                p_sends[d].start()
    drain(d_recv.at[pl.ds(1, tp - 1)], dr_sem)
    dsum = dec_own.astype(F32)
    for d in order:
        dsum = dsum + d_recv[d].astype(F32)
    out[rows:, :] = jnp.broadcast_to(dsum, (out.shape[0] - rows, cols)).astype(BF16) if (
        drows == 1
    ) else jnp.concatenate(
        [dsum, jnp.zeros((out.shape[0] - rows - drows, cols), F32)], axis=0
    ).astype(BF16)
    drain(q_all.at[pl.ds(0, kv - 1)], qs_sem)
    drain(st_send.at[pl.ds(0, kv - 1)], ss_sem)
    drain(att_send.at[:, pl.ds(0, kv - 1)], as_sem)
    drain(d_send.at[pl.ds(1, tp - 1)], ds_sem)
    drain(p_send.at[pl.ds(1, tp - 1)], ps_sem)
    drain(p_recv.at[pl.ds(1, tp - 1)], pr_sem)
    for d in order:
        own = own + p_recv[d].astype(F32)
    out[0:rows, :] = own.astype(BF16)


def body(
    tokens, dec_tokens, norm_gain, w_query, w_key, w_value, w_out, head_gain, mix_lambda,
    ctx_keys, ctx_values, dec_keys, dec_values, dec_len, *, kv, tp,
):
    rows, width = tokens.shape
    drows = dec_tokens.shape[0]
    w = w_query.shape[2]
    heads = w // DH
    vwid = w_value.shape[1]
    ctx = ctx_keys.shape[1]
    slots = dec_keys.shape[2]
    cols = w_out.shape[1] // tp
    padded = rows + -(-drows // 16) * 16
    blocks = rows * kv // piece_block(rows * kv)
    any_spec = pl.BlockSpec(memory_space=pltpu.HBM)
    vmem = pl.BlockSpec(memory_space=pltpu.VMEM)
    dma = pltpu.SemaphoreType.DMA
    V = pltpu.VMEM

    def hbm(x):
        return pltpu.with_memory_space_constraint(x, pltpu.HBM) if x.size > 1 else x

    out = pl.pallas_call(
        functools.partial(kernel, kv, tp),
        out_shape=jax.ShapeDtypeStruct((padded, cols), BF16),
        in_specs=[any_spec] * 8 + [pl.BlockSpec(memory_space=pl.ANY)] * 2 + [any_spec] * 4,
        out_specs=vmem,
        scratch_shapes=[
            pltpu.SMEM((heads,), F32), pltpu.SMEM((drows,), jnp.int32),
            V((rows, width), BF16), V((drows, width), BF16), V((1, width), F32),
            V((1, 2 * DH), F32),
            V((2, width, w), BF16), V((2, width, w), BF16), V((width, vwid), BF16),
            V((tp, vwid, cols), BF16),
            V((2, ctx, w), BF16), V((ctx, vwid), BF16),
            V((2, drows, slots, w), BF16), V((drows, slots, vwid), BF16),
            V((padded, width), BF16), V((kv, rows, 2 * w), BF16),
            V((2, LANES, w), BF16), V((LANES, vwid), BF16),
            V((kv, 1, LANES), F32), V((kv, 1, LANES), F32),
            V((2 * heads, kv, rows, LANES), F32),
            V((heads, kv, rows, 4 * DH), BF16), V((heads, kv, rows, 4 * DH), BF16),
            V((tp, rows, cols), F32),
            V((tp, rows, cols), BF16), V((tp, rows, cols), BF16),
            V((tp, drows, cols), BF16), V((tp, drows, cols), BF16),
            dma((6,)), dma((Q_PARTS,)), dma((K_PARTS,)), dma((V_PARTS,)), dma((tp,)),
            dma((2,)), dma((2,)),
            dma(()), dma((blocks,)), dma(()), dma(()), dma(()), dma((heads,)),
            dma(()), dma(()), dma(()), dma(()),
        ],
        compiler_params=pltpu.CompilerParams(
            collective_id=0, has_side_effects=True, vmem_limit_bytes=48 * 1024 * 1024
        ),
    )(
        hbm(tokens), hbm(dec_tokens), hbm(norm_gain.reshape(1, width)), hbm(w_query),
        hbm(w_key), hbm(w_value), hbm(w_out), hbm(head_gain.reshape(1, 2 * DH)),
        hbm(mix_lambda), hbm(dec_len), hbm(ctx_keys), hbm(ctx_values), hbm(dec_keys),
        hbm(dec_values),
    )

    def split(src, piece_ref, dec_ref):
        piece_ref[...] = src[0:rows, :]
        dec_ref[...] = src[rows : rows + drows, :]

    return pl.pallas_call(
        split,
        out_shape=(
            jax.ShapeDtypeStruct((rows, cols), BF16),
            jax.ShapeDtypeStruct((drows, cols), BF16),
        ),
        in_specs=[vmem],
        out_specs=(vmem, vmem),
        compiler_params=pltpu.CompilerParams(vmem_limit_bytes=1024 * 1024),
    )(out)


def solution(mesh):
    in_specs = (
        P("kv", None),
        P("kv", None),
        P(),
        P(None, None, "tp"),
        P(None, None, "tp"),
        P(None, "tp"),
        P("tp", None),
        P(),
        P("tp"),
        P(None, "kv", "tp"),
        P("kv", "tp"),
        P(None, "kv", None, "tp"),
        P("kv", None, "tp"),
        P("kv"),
    )
    out_specs = (P("kv", "tp"), P("kv", "tp"))
    step = functools.partial(body, kv=mesh.shape["kv"], tp=mesh.shape["tp"])
    return jax.shard_map(step, mesh=mesh, in_specs=in_specs, out_specs=out_specs, check_vma=False)
```

```python
import functools
import math

import jax
import jax.numpy as jnp
from jax import lax
from jax.experimental import pallas as pl
from jax.experimental.pallas import tpu as pltpu
from jax.sharding import PartitionSpec as P

DH = 128
epsilon = 1e-06
MESH = pl.DeviceIdType.MESH
F32 = jnp.float32
BF16 = jnp.bfloat16
LANES = 128
C_EXP = DH ** (-0.5) * math.log2(math.e)
Q_PARTS = 8
K_PARTS = 2
BLOCK = 64
UNROLL = 8
UNIT = 2
V_PARTS = 2


def dot(a, b):
    return jnp.dot(a, b, preferred_element_type=F32)


def dot_nt(a, b):
    return lax.dot_general(a, b, (((1,), (1,)), ((), ())), preferred_element_type=F32)


def piece_block(total):
    return BLOCK if total % BLOCK == 0 else LANES


def kernel(
    kv, tp,
    tokens, dec_tokens, norm_gain, w_query, w_key, w_value, w_out, head_gain,
    mix_lambda, dec_len, ctx_keys, ctx_values, dec_keys, dec_values,
    out,
    lam_s, len_s, tok_v, dtok_v, gain_v, hgain_v, wq_v, wk_v, wv_v, wo_v,
    ck_v, cv_v, dk_v, dv_v,
    kt_v, kn_v, xs, q_all, kown, vown, st_send, st_recv, fac_v, att_send, att_recv, p_send, p_recv,
    d_send, d_recv,
    sem_small, sem_q, sem_k, sem_v, sem_o, sem_c, sem_d,
    qs_sem, qr_sem, ss_sem, sr_sem, as_sem, ar_sem, ps_sem, pr_sem, ds_sem, dr_sem,
):
    me = lax.axis_index("kv")
    mt = lax.axis_index("tp")
    rows, width = tokens.shape
    drows = dec_tokens.shape[0]
    w = w_query.shape[2]
    heads = w // DH
    vw = 2 * DH
    slots = dec_keys.shape[2]
    total = rows * kv
    cols = w_out.shape[1] // tp
    block = piece_block(total)
    blocks = total // block
    padded = xs.shape[0]
    per = block // rows

    def tp_peer(d):
        chip = lax.rem(mt // 2 + d // 2, tp // 2)
        return chip * 2 + lax.rem(mt + d, 2)

    barrier = pltpu.get_barrier_semaphore()
    for d in range(1, kv):
        pl.semaphore_signal(
            barrier, inc=1, device_id=(lax.rem(me + d, kv), mt), device_id_type=MESH
        )
    for d in range(1, tp):
        pl.semaphore_signal(
            barrier, inc=1, device_id=(me, tp_peer(d)), device_id_type=MESH
        )

    small = [
        pltpu.make_async_copy(tokens, tok_v, sem_small.at[0]),
        pltpu.make_async_copy(dec_tokens, dtok_v, sem_small.at[1]),
        pltpu.make_async_copy(norm_gain, gain_v, sem_small.at[2]),
        pltpu.make_async_copy(head_gain, hgain_v, sem_small.at[3]),
        pltpu.make_async_copy(mix_lambda, lam_s, sem_small.at[4]),
        pltpu.make_async_copy(dec_len, len_s, sem_small.at[5]),
    ]
    for c in small:
        c.start()

    qstep = width // Q_PARTS
    kstep = width // K_PARTS
    vstep = width // V_PARTS
    q_copies = []
    for i in range(Q_PARTS):
        sl = (slice(None), pl.ds(i * qstep, qstep))
        q_copies.append(pltpu.make_async_copy(w_query.at[sl], wq_v.at[sl], sem_q.at[i]))
    k_copies = []
    for i in range(K_PARTS):
        sl = (slice(None), pl.ds(i * kstep, kstep))
        k_copies.append(pltpu.make_async_copy(w_key.at[sl], wk_v.at[sl], sem_k.at[i]))
    v_copies = [
        pltpu.make_async_copy(
            w_value.at[pl.ds(i * vstep, vstep)], wv_v.at[pl.ds(i * vstep, vstep)], sem_v.at[i]
        )
        for i in range(V_PARTS)
    ]
    ck_copy = pltpu.make_async_copy(ctx_keys, ck_v, sem_c.at[0])
    cv_copy = pltpu.make_async_copy(ctx_values, cv_v, sem_c.at[1])
    dk_copy = pltpu.make_async_copy(dec_keys, dk_v, sem_d.at[0])
    dv_copy = pltpu.make_async_copy(dec_values, dv_v, sem_d.at[1])
    wo_copies = []
    for d in range(tp):
        start = pl.multiple_of(tp_peer(d) * cols, LANES)
        wo_copies.append(
            pltpu.make_async_copy(w_out.at[:, pl.ds(start, cols)], wo_v.at[d], sem_o)
        )
    for c in q_copies:
        c.start(priority=1)

    kown[...] = jnp.zeros_like(kown)
    vown[...] = jnp.zeros_like(vown)
    xs[rows:, :] = jnp.zeros((padded - rows, width), BF16)
    for c in small[:3]:
        c.wait()
    gain = gain_v[...]

    def normed(x):
        xf = x.astype(F32)
        inv = lax.rsqrt(jnp.mean(xf * xf, axis=-1, keepdims=True) + epsilon)
        return (xf * inv * gain).astype(BF16)

    xs[0:rows, :] = normed(tok_v[...])
    xs[rows : rows + drows, :] = normed(dtok_v[...])

    def to_kv(src, dst, send, recv, d):
        return pltpu.make_async_remote_copy(
            src_ref=src, dst_ref=dst, send_sem=send, recv_sem=recv,
            device_id=(lax.rem(me + d + kv, kv), mt), device_id_type=MESH,
        )

    def drain(ref, sem):
        pltpu.make_async_copy(ref, ref, sem).wait()

    def far_peer(i):
        down = kv - 1 - i - jnp.where(kv - 1 - i <= me, 1, 0)
        up = i + jnp.where(i >= me, 1, 0)
        return jnp.where(2 * me < kv, down, up)

    for c in k_copies + [ck_copy]:
        c.start(priority=1)
    acc = [None, None]
    for i in range(Q_PARTS):
        q_copies[i].wait()
        sl = slice(i * qstep, (i + 1) * qstep)
        for c in range(2):
            term = dot(xs[:, sl], wq_v[c, sl, :])
            acc[c] = term if acc[c] is None else acc[c] + term
    dec_q = []
    for c in range(2):
        qc = acc[c].astype(BF16)
        q_all[me, :, c * w : (c + 1) * w] = qc[0:rows]
        dec_q.append(qc[rows:])
    for c in v_copies + [cv_copy]:
        c.start(priority=1)
    pl.semaphore_wait(barrier, kv + tp - 2)
    for i in range(kv - 1):
        ring = sorted(range(1, kv), key=lambda d: (-min(d, kv - d), d))[i]
        half = kv // 2
        if i < half:
            up_first = half + i - me
        else:
            near = i - half
            up_first = near + jnp.where(near >= me, 1, 0) - me
        d = jnp.where(me < half, up_first, ring)
        to_kv(q_all.at[me], q_all.at[me], qs_sem, qr_sem.at[lax.div(me, UNIT)], d).start()

    acc = [None, None]
    for i in range(K_PARTS):
        k_copies[i].wait()
        sl = slice(i * kstep, (i + 1) * kstep)
        for c in range(2):
            term = dot(xs[:, sl], wk_v[c, sl, :])
            acc[c] = term if acc[c] is None else acc[c] + term
    dec_k = []
    for c in range(2):
        kc = acc[c].astype(BF16)
        kown[c, 0:rows, :] = kc[0:rows]
        dec_k.append(kc[rows:])
    ck_copy.wait()
    for c in range(2):
        kt_v[c] = jnp.transpose(ck_v[c])
        kn_v[c] = jnp.transpose(kown[c])
    for c in [dk_copy, dv_copy]:
        c.start(priority=1)
    acc = None
    for i in range(V_PARTS):
        v_copies[i].wait()
        term = dot(xs[:, i * vstep : (i + 1) * vstep], wv_v[i * vstep : (i + 1) * vstep, :])
        acc = term if acc is None else acc + term
    vc = acc.astype(BF16)
    vown[0:rows, :] = vc[0:rows]
    dec_v = vc[rows:]
    for c in wo_copies:
        c.start(priority=1)

    cv_copy.wait()
    nstat = 4 * heads
    most = LANES // rows

    def wait_queries(u):
        inside = lax.div(me, UNIT) == u

        @pl.when(inside)
        def _():
            drain(q_all.at[pl.ds(u * UNIT, UNIT - 1)], qr_sem.at[u])

        @pl.when(jnp.logical_not(inside))
        def _():
            drain(q_all.at[pl.ds(u * UNIT, UNIT)], qr_sem.at[u])

    def attend(first, per):
        block = per * rows
        slots_b = pl.ds(first, per)
        qb = q_all[slots_b].reshape(block, 2 * w)
        pos = first * rows + lax.broadcasted_iota(jnp.int32, (block, LANES), 0)
        lane = lax.broadcasted_iota(jnp.int32, (block, LANES), 1)
        ok = (lane < rows) & (lane + me * rows <= pos)
        ok = jnp.concatenate([ok] * heads, axis=0) if heads > 1 else ok
        head_of = lax.broadcasted_iota(jnp.int32, (block, w), 1) // DH
        stats = jnp.zeros((block, LANES), F32)
        far_p = []
        near_p = []
        for c in range(2):
            qc = qb[:, c * w : (c + 1) * w]
            if heads > 1:
                zero = jnp.zeros_like(qc)
                qc = jnp.concatenate(
                    [jnp.where(head_of == h, qc, zero) for h in range(heads)], axis=0
                )
            far = dot(qc, kt_v[c])
            near = dot(qc, kn_v[c])
            near = jnp.where(ok, near, -jnp.inf)
            top = jnp.maximum(
                jnp.max(far, axis=-1, keepdims=True), jnp.max(near, axis=-1, keepdims=True)
            )
            ef = jnp.exp2((far - top) * C_EXP)
            en = jnp.exp2((near - top) * C_EXP)
            tot = jnp.sum(ef, axis=-1, keepdims=True) + jnp.sum(en, axis=-1, keepdims=True)
            far_p.append(ef.astype(BF16))
            near_p.append(en.astype(BF16))
            for h in range(heads):
                part = slice(h * block, (h + 1) * block)
                stats = jnp.where(lane == 2 * h + c, top[part], stats)
                stats = jnp.where(lane == 2 * heads + 2 * h + c, tot[part], stats)
        for h in range(heads):
            part = slice(h * block, (h + 1) * block)
            hv = slice(h * vw, (h + 1) * vw)
            att = dot(jnp.concatenate([p[part] for p in far_p], axis=0), cv_v[:, hv]) + dot(
                jnp.concatenate([p[part] for p in near_p], axis=0), vown[:, hv]
            )
            for c in range(2):
                att_send[h, slots_b, :, c * vw : (c + 1) * vw] = (
                    att[c * block : (c + 1) * block].astype(BF16).reshape(per, rows, vw)
                )
        if block < LANES:
            stats = jnp.concatenate([stats, jnp.zeros((LANES - block, LANES), F32)], axis=0)
        by_row = jnp.transpose(stats)
        group_of = lax.broadcasted_iota(jnp.int32, (most, LANES), 1) // rows
        packed = jnp.zeros((most, LANES), F32)
        for s in range(nstat):
            line = jnp.broadcast_to(by_row[s : s + 1, :], (most, LANES))
            line = pltpu.roll(line, rows, 1, stride=rows, stride_axis=0)
            if s:
                line = pltpu.roll(line, s * rows, 1)
            packed = jnp.where(group_of == s, line, packed)
        for o in range(per):
            st_send[first + o] = packed[most - 1 - o : most - o, :]

    def send_block(peers):
        for peer in peers:
            d = lax.rem(peer - me + kv, kv)

            @pl.when(peer != me)
            def _(peer=peer, d=d):
                to_kv(st_send.at[peer], st_recv.at[d], ss_sem, sr_sem, d).start()

        for peer in peers:
            d = lax.rem(peer - me + kv, kv)

            @pl.when(peer != me)
            def _(peer=peer, d=d):
                for h in range(heads):
                    to_kv(
                        att_send.at[h, peer], att_recv.at[h, d], as_sem, ar_sem, d
                    ).start()

    units = kv // UNIT
    if kv <= UNROLL:
        quarter, half = kv // 4, kv // 2
        for first, count, peers in (
            (0, quarter, range(quarter)),
            (quarter, half - quarter, range(quarter, half)),
            (half, kv - half, range(half, kv)),
        ):
            for u in range(first // UNIT, (first + count) // UNIT):
                wait_queries(u)
            attend(first, count)
            send_block(peers)
    else:
        for u in range(units):
            wait_queries(u)
        pl.loop(0, blocks)(lambda b: attend(b * per, per))
        send_block(range(kv))
    st_recv[0] = st_send[me]

    for c in small[3:]:
        c.wait()
    hgain = hgain_v[...]
    group = 16
    hrow = lax.broadcasted_iota(jnp.int32, (group, w), 0)
    hcol = lax.broadcasted_iota(jnp.int32, (group, w), 1) // DH
    own_head = hrow == hcol
    row1 = lax.broadcasted_iota(jnp.int32, (group, 1), 0)
    lam_col = jnp.zeros((group, 1), F32)
    for h in range(heads):
        lam_col = jnp.where(row1 == h, lam_s[h], lam_col)
    dk_copy.wait()
    slot_id = lax.broadcasted_iota(jnp.int32, (group, slots), 1)
    vrow = lax.broadcasted_iota(jnp.int32, (group, heads * vw), 0)
    vcol = lax.broadcasted_iota(jnp.int32, (group, heads * vw), 1) // vw
    dec_att = []
    for r in range(drows):
        far_p = []
        near_p = []
        for c in range(2):
            qr = jnp.broadcast_to(dec_q[c][r : r + 1].astype(F32), (group, w))
            qr = jnp.where(own_head, qr, 0.0)
            kr = dec_k[c][r : r + 1].astype(F32)
            near = jnp.sum(qr * kr, axis=-1, keepdims=True)
            far = dot_nt(qr.astype(BF16), dk_v[c, r])
            far = jnp.where(slot_id < len_s[r], far, -jnp.inf)
            top = jnp.maximum(jnp.max(far, axis=-1, keepdims=True), near)
            ef = jnp.exp2((far - top) * C_EXP)
            en = jnp.exp2((near - top) * C_EXP)
            den = jnp.sum(ef, axis=-1, keepdims=True) + en
            far_p.append(ef / den)
            near_p.append(en / den)
        far_w = (far_p[0] - lam_col * far_p[1]).astype(BF16)
        near_w = (near_p[0] - lam_col * near_p[1]).astype(BF16).astype(F32)
        if r == 0:
            dv_copy.wait()
        att = dot(far_w, dv_v[r]) + near_w * dec_v[r : r + 1].astype(F32)
        dec_att.append(jnp.sum(jnp.where(vrow == vcol, att, 0.0), axis=0, keepdims=True))

    def head_norm(att):
        inv = lax.rsqrt(jnp.mean(att * att, axis=-1, keepdims=True) + epsilon)
        return (att * inv * hgain).astype(BF16)

    def to_tp(src, dst, send, recv, d):
        return pltpu.make_async_remote_copy(
            src_ref=src.at[d], dst_ref=dst.at[d], send_sem=send, recv_sem=recv,
            device_id=(me, tp_peer(d)), device_id_type=MESH,
        )

    def out_part(ho, d, h):
        return dot(ho, wo_v[d, h * vw : (h + 1) * vw, :])

    dec_rows = jnp.concatenate(dec_att, axis=0) if drows > 1 else dec_att[0]
    dec_rows = dec_rows if drows > 1 else jnp.broadcast_to(dec_rows, (group, heads * vw))
    dec_ho = [head_norm(dec_rows[:, h * vw : (h + 1) * vw]) for h in range(heads)]
    drain(wo_v, sem_o)
    order = sorted(range(1, tp), key=lambda d: (d < 2, d))

    def dec_project(d):
        acc = None
        for h in range(heads):
            term = out_part(dec_ho[h], d, h)
            acc = term if acc is None else acc + term
        return acc[0:drows].astype(BF16)

    d_sends = {d: to_tp(d_send, d_recv, ds_sem, dr_sem, d) for d in order}
    for d in order:
        d_send[d] = dec_project(d)
        d_sends[d].start()
    dec_own = dec_project(0)

    lane = lax.broadcasted_iota(jnp.int32, (1, LANES), 1)
    p_sends = {d: to_tp(p_send, p_recv, ps_sem, pr_sem, d) for d in order}
    drain(st_recv.at[pl.ds(1, kv - 1)], sr_sem)
    nmax = 2 * heads * rows
    sts = st_recv[...].reshape(kv, LANES)
    top = jnp.max(sts, axis=0, keepdims=True)
    fac = jnp.exp2((sts - top) * C_EXP)
    den = jnp.sum(fac * pltpu.roll(sts, LANES - nmax, 1), axis=0, keepdims=True)
    den = jnp.where(lane < nmax, den, 1.0)
    sign = jnp.ones((1, LANES), F32)
    for h in range(heads):
        sign = jnp.where(lane // rows == 2 * h + 1, -lam_s[h], sign)
    fac = jnp.transpose(fac * (sign / den))
    for i in range(2 * heads):
        for d in range(kv):
            fac_v[i, d] = jnp.broadcast_to(
                fac[i * rows : (i + 1) * rows, d : d + 1], (rows, LANES)
            )
    drain(att_recv.at[:, pl.ds(1, kv - 1)], ar_sem)
    ho = []
    for h in range(heads):
        total_att = None
        for d in range(kv):
            blk = att_send[h, me] if d == 0 else att_recv[h, d]
            for c in range(2):
                f = fac_v[2 * h + c, d]
                term = jnp.concatenate([f] * (vw // LANES), axis=1) * blk[
                    :, c * vw : (c + 1) * vw
                ].astype(F32)
                total_att = term if total_att is None else total_att + term
        ho.append(head_norm(total_att))
    ho = jnp.concatenate(ho, axis=1) if heads > 1 else ho[0]
    for group_d in (order[:1], order[1:] + [0]):
        for d in group_d:
            term = dot(ho, wo_v[d]).astype(BF16)
            if d > 0:
                p_send[d] = term
            else:
                own = term.astype(F32)
        for d in group_d:
            if d > 0:
                p_sends[d].start()
    drain(d_recv.at[pl.ds(1, tp - 1)], dr_sem)
    dsum = dec_own.astype(F32)
    for d in order:
        dsum = dsum + d_recv[d].astype(F32)
    out[rows:, :] = jnp.broadcast_to(dsum, (out.shape[0] - rows, cols)).astype(BF16) if (
        drows == 1
    ) else jnp.concatenate(
        [dsum, jnp.zeros((out.shape[0] - rows - drows, cols), F32)], axis=0
    ).astype(BF16)
    drain(q_all.at[pl.ds(0, kv - 1)], qs_sem)
    drain(st_send.at[pl.ds(0, kv - 1)], ss_sem)
    drain(att_send.at[:, pl.ds(0, kv - 1)], as_sem)
    drain(d_send.at[pl.ds(1, tp - 1)], ds_sem)
    drain(p_send.at[pl.ds(1, tp - 1)], ps_sem)
    drain(p_recv.at[pl.ds(1, tp - 1)], pr_sem)
    for d in order:
        own = own + p_recv[d].astype(F32)
    out[0:rows, :] = own.astype(BF16)


def body(
    tokens, dec_tokens, norm_gain, w_query, w_key, w_value, w_out, head_gain, mix_lambda,
    ctx_keys, ctx_values, dec_keys, dec_values, dec_len, *, kv, tp,
):
    rows, width = tokens.shape
    drows = dec_tokens.shape[0]
    w = w_query.shape[2]
    heads = w // DH
    vwid = w_value.shape[1]
    ctx = ctx_keys.shape[1]
    slots = dec_keys.shape[2]
    cols = w_out.shape[1] // tp
    padded = rows + -(-drows // 16) * 16
    any_spec = pl.BlockSpec(memory_space=pltpu.HBM)
    vmem = pl.BlockSpec(memory_space=pltpu.VMEM)
    dma = pltpu.SemaphoreType.DMA
    V = pltpu.VMEM

    def hbm(x):
        return pltpu.with_memory_space_constraint(x, pltpu.HBM) if x.size > 1 else x

    out = pl.pallas_call(
        functools.partial(kernel, kv, tp),
        out_shape=jax.ShapeDtypeStruct((padded, cols), BF16),
        in_specs=[any_spec] * 8 + [pl.BlockSpec(memory_space=pl.ANY)] * 2 + [any_spec] * 4,
        out_specs=vmem,
        scratch_shapes=[
            pltpu.SMEM((heads,), F32), pltpu.SMEM((drows,), jnp.int32),
            V((rows, width), BF16), V((drows, width), BF16), V((1, width), F32),
            V((1, 2 * DH), F32),
            V((2, width, w), BF16), V((2, width, w), BF16), V((width, vwid), BF16),
            V((tp, vwid, cols), BF16),
            V((2, ctx, w), BF16), V((ctx, vwid), BF16),
            V((2, drows, slots, w), BF16), V((drows, slots, vwid), BF16),
            V((2, w, ctx), BF16), V((2, w, LANES), BF16),
            V((padded, width), BF16), V((kv, rows, 2 * w), BF16),
            V((2, LANES, w), BF16), V((LANES, vwid), BF16),
            V((kv, 1, LANES), F32), V((kv, 1, LANES), F32),
            V((2 * heads, kv, rows, LANES), F32),
            V((heads, kv, rows, 4 * DH), BF16), V((heads, kv, rows, 4 * DH), BF16),
            V((tp, rows, cols), BF16), V((tp, rows, cols), BF16),
            V((tp, drows, cols), BF16), V((tp, drows, cols), BF16),
            dma((6,)), dma((Q_PARTS,)), dma((K_PARTS,)), dma((V_PARTS,)), dma(()),
            dma((2,)), dma((2,)),
            dma(()), dma((kv // UNIT,)), dma(()), dma(()), dma(()), dma(()),
            dma(()), dma(()), dma(()), dma(()),
        ],
        compiler_params=pltpu.CompilerParams(
            collective_id=0, has_side_effects=True, vmem_limit_bytes=48 * 1024 * 1024
        ),
    )(
        hbm(tokens), hbm(dec_tokens), hbm(norm_gain.reshape(1, width)), hbm(w_query),
        hbm(w_key), hbm(w_value), hbm(w_out), hbm(head_gain.reshape(1, 2 * DH)),
        hbm(mix_lambda), hbm(dec_len), hbm(ctx_keys), hbm(ctx_values), hbm(dec_keys),
        hbm(dec_values),
    )

    def split(src, piece_ref, dec_ref):
        piece_ref[...] = src[0:rows, :]
        dec_ref[...] = src[rows : rows + drows, :]

    return pl.pallas_call(
        split,
        out_shape=(
            jax.ShapeDtypeStruct((rows, cols), BF16),
            jax.ShapeDtypeStruct((drows, cols), BF16),
        ),
        in_specs=[vmem],
        out_specs=(vmem, vmem),
        compiler_params=pltpu.CompilerParams(vmem_limit_bytes=1024 * 1024),
    )(out)


def solution(mesh):
    in_specs = (
        P("kv", None),
        P("kv", None),
        P(),
        P(None, None, "tp"),
        P(None, None, "tp"),
        P(None, "tp"),
        P("tp", None),
        P(),
        P("tp"),
        P(None, "kv", "tp"),
        P("kv", "tp"),
        P(None, "kv", None, "tp"),
        P("kv", None, "tp"),
        P("kv"),
    )
    out_specs = (P("kv", "tp"), P("kv", "tp"))
    step = functools.partial(body, kv=mesh.shape["kv"], tp=mesh.shape["tp"])
    return jax.shard_map(step, mesh=mesh, in_specs=in_specs, out_specs=out_specs, check_vma=False)
```

```python
import functools
import math

import jax
import jax.numpy as jnp
from jax import lax
from jax.experimental import pallas as pl
from jax.experimental.pallas import tpu as pltpu
from jax.sharding import PartitionSpec as P

DH = 128
epsilon = 1e-06
MESH = pl.DeviceIdType.MESH
F32 = jnp.float32
BF16 = jnp.bfloat16
LANES = 128
C_EXP = DH ** (-0.5) * math.log2(math.e)
Q_PARTS = 8
K_PARTS = 2
BLOCK = 64
UNROLL = 8
UNIT = 2
V_PARTS = 2


def dot(a, b):
    return jnp.dot(a, b, preferred_element_type=F32)


def dot_nt(a, b):
    return lax.dot_general(a, b, (((1,), (1,)), ((), ())), preferred_element_type=F32)


def piece_block(total):
    return BLOCK if total % BLOCK == 0 else LANES


def kernel(
    kv, tp,
    tokens, dec_tokens, norm_gain, w_query, w_key, w_value, w_out, head_gain,
    mix_lambda, dec_len, ctx_keys, ctx_values, dec_keys, dec_values,
    out,
    lam_s, len_s, tok_v, dtok_v, gain_v, hgain_v, wq_v, wk_v, wv_v, wo_v,
    ck_v, cv_v, dk_v, dv_v,
    kt_v, kn_v, xs, q_all, kown, vown, st_send, st_recv, fac_v, att_send, att_recv, p_send, p_recv,
    d_send, d_recv,
    sem_small, sem_q, sem_k, sem_v, sem_o, sem_c, sem_d,
    qs_sem, qr_sem, ss_sem, sr_sem, as_sem, ar_sem, ps_sem, pr_sem, ds_sem, dr_sem,
):
    me = lax.axis_index("kv")
    mt = lax.axis_index("tp")
    rows, width = tokens.shape
    drows = dec_tokens.shape[0]
    w = w_query.shape[2]
    heads = w // DH
    vw = 2 * DH
    slots = dec_keys.shape[2]
    total = rows * kv
    cols = w_out.shape[1] // tp
    block = piece_block(total)
    blocks = total // block
    padded = xs.shape[0]
    per = block // rows

    def tp_peer(d):
        chip = lax.rem(mt // 2 + d // 2, tp // 2)
        return chip * 2 + lax.rem(mt + d, 2)

    barrier = pltpu.get_barrier_semaphore()
    for d in range(1, kv):
        pl.semaphore_signal(
            barrier, inc=1, device_id=(lax.rem(me + d, kv), mt), device_id_type=MESH
        )
    for d in range(1, tp):
        pl.semaphore_signal(
            barrier, inc=1, device_id=(me, tp_peer(d)), device_id_type=MESH
        )

    small = [
        pltpu.make_async_copy(tokens, tok_v, sem_small.at[0]),
        pltpu.make_async_copy(dec_tokens, dtok_v, sem_small.at[1]),
        pltpu.make_async_copy(norm_gain, gain_v, sem_small.at[2]),
        pltpu.make_async_copy(head_gain, hgain_v, sem_small.at[3]),
        pltpu.make_async_copy(mix_lambda, lam_s, sem_small.at[4]),
        pltpu.make_async_copy(dec_len, len_s, sem_small.at[5]),
    ]
    for c in small:
        c.start()

    qstep = width // Q_PARTS
    kstep = width // K_PARTS
    vstep = width // V_PARTS
    q_copies = []
    for i in range(Q_PARTS):
        sl = (slice(None), pl.ds(i * qstep, qstep))
        q_copies.append(pltpu.make_async_copy(w_query.at[sl], wq_v.at[sl], sem_q.at[i]))
    k_copies = []
    for i in range(K_PARTS):
        sl = (slice(None), pl.ds(i * kstep, kstep))
        k_copies.append(pltpu.make_async_copy(w_key.at[sl], wk_v.at[sl], sem_k.at[i]))
    v_copies = [
        pltpu.make_async_copy(
            w_value.at[pl.ds(i * vstep, vstep)], wv_v.at[pl.ds(i * vstep, vstep)], sem_v.at[i]
        )
        for i in range(V_PARTS)
    ]
    ck_copy = pltpu.make_async_copy(ctx_keys, ck_v, sem_c.at[0])
    cv_copy = pltpu.make_async_copy(ctx_values, cv_v, sem_c.at[1])
    dk_copy = pltpu.make_async_copy(dec_keys, dk_v, sem_d.at[0])
    dv_copy = pltpu.make_async_copy(dec_values, dv_v, sem_d.at[1])
    wo_copies = []
    for d in range(tp):
        start = pl.multiple_of(tp_peer(d) * cols, LANES)
        wo_copies.append(
            pltpu.make_async_copy(w_out.at[:, pl.ds(start, cols)], wo_v.at[d], sem_o)
        )
    for c in q_copies:
        c.start(priority=1)

    kown[...] = jnp.zeros_like(kown)
    vown[...] = jnp.zeros_like(vown)
    xs[rows:, :] = jnp.zeros((padded - rows, width), BF16)
    for c in small[:3]:
        c.wait()
    gain = gain_v[...]

    def normed(x):
        xf = x.astype(F32)
        inv = lax.rsqrt(jnp.mean(xf * xf, axis=-1, keepdims=True) + epsilon)
        return (xf * inv * gain).astype(BF16)

    xs[0:rows, :] = normed(tok_v[...])
    xs[rows : rows + drows, :] = normed(dtok_v[...])

    def to_kv(src, dst, send, recv, d):
        return pltpu.make_async_remote_copy(
            src_ref=src, dst_ref=dst, send_sem=send, recv_sem=recv,
            device_id=(lax.rem(me + d + kv, kv), mt), device_id_type=MESH,
        )

    def drain(ref, sem):
        pltpu.make_async_copy(ref, ref, sem).wait()

    for c in k_copies + [ck_copy]:
        c.start(priority=1)
    acc = [None, None]
    for i in range(Q_PARTS):
        q_copies[i].wait()
        sl = slice(i * qstep, (i + 1) * qstep)
        for c in range(2):
            term = dot(xs[:, sl], wq_v[c, sl, :])
            acc[c] = term if acc[c] is None else acc[c] + term
    dec_q = []
    for c in range(2):
        qc = acc[c].astype(BF16)
        q_all[me, :, c * w : (c + 1) * w] = qc[0:rows]
        dec_q.append(qc[rows:])
    for c in v_copies + [cv_copy]:
        c.start(priority=1)
    pl.semaphore_wait(barrier, kv + tp - 2)
    for i in range(kv - 1):
        ring = sorted(range(1, kv), key=lambda d: (-min(d, kv - d), d))[i]
        half = kv // 2
        if i < half:
            up_first = half + (i ^ 1 if half % 2 == 0 else i) - me
        else:
            near = i - half
            up_first = near + jnp.where(near >= me, 1, 0) - me
        d = jnp.where(me < half, up_first, ring)
        to_kv(q_all.at[me], q_all.at[me], qs_sem, qr_sem.at[lax.div(me, UNIT)], d).start()

    acc = [None, None]
    for i in range(K_PARTS):
        k_copies[i].wait()
        sl = slice(i * kstep, (i + 1) * kstep)
        for c in range(2):
            term = dot(xs[:, sl], wk_v[c, sl, :])
            acc[c] = term if acc[c] is None else acc[c] + term
    dec_k = []
    for c in range(2):
        kc = acc[c].astype(BF16)
        kown[c, 0:rows, :] = kc[0:rows]
        dec_k.append(kc[rows:])
    ck_copy.wait()
    for c in range(2):
        kt_v[c] = jnp.transpose(ck_v[c])
        kn_v[c] = jnp.transpose(kown[c])
    for c in [dk_copy, dv_copy]:
        c.start(priority=1)
    acc = None
    for i in range(V_PARTS):
        v_copies[i].wait()
        term = dot(xs[:, i * vstep : (i + 1) * vstep], wv_v[i * vstep : (i + 1) * vstep, :])
        acc = term if acc is None else acc + term
    vc = acc.astype(BF16)
    vown[0:rows, :] = vc[0:rows]
    dec_v = vc[rows:]
    for c in wo_copies:
        c.start(priority=1)

    cv_copy.wait()
    nstat = 4 * heads
    most = LANES // rows

    def wait_queries(u):
        inside = lax.div(me, UNIT) == u

        @pl.when(inside)
        def _():
            drain(q_all.at[pl.ds(u * UNIT, UNIT - 1)], qr_sem.at[u])

        @pl.when(jnp.logical_not(inside))
        def _():
            drain(q_all.at[pl.ds(u * UNIT, UNIT)], qr_sem.at[u])

    def attend(first, per):
        block = per * rows
        slots_b = pl.ds(first, per)
        qb = q_all[slots_b].reshape(block, 2 * w)
        pos = first * rows + lax.broadcasted_iota(jnp.int32, (block, LANES), 0)
        lane = lax.broadcasted_iota(jnp.int32, (block, LANES), 1)
        ok = (lane < rows) & (lane + me * rows <= pos)
        ok = jnp.concatenate([ok] * heads, axis=0) if heads > 1 else ok
        head_of = lax.broadcasted_iota(jnp.int32, (block, w), 1) // DH
        stats = jnp.zeros((block, LANES), F32)
        far_p = []
        near_p = []
        for c in range(2):
            qc = qb[:, c * w : (c + 1) * w]
            if heads > 1:
                zero = jnp.zeros_like(qc)
                qc = jnp.concatenate(
                    [jnp.where(head_of == h, qc, zero) for h in range(heads)], axis=0
                )
            far = dot(qc, kt_v[c])
            near = dot(qc, kn_v[c])
            near = jnp.where(ok, near, -jnp.inf)
            top = jnp.maximum(
                jnp.max(far, axis=-1, keepdims=True), jnp.max(near, axis=-1, keepdims=True)
            )
            ef = jnp.exp2((far - top) * C_EXP)
            en = jnp.exp2((near - top) * C_EXP)
            tot = jnp.sum(ef, axis=-1, keepdims=True) + jnp.sum(en, axis=-1, keepdims=True)
            far_p.append(ef.astype(BF16))
            near_p.append(en.astype(BF16))
            for h in range(heads):
                part = slice(h * block, (h + 1) * block)
                stats = jnp.where(lane == 2 * h + c, top[part], stats)
                stats = jnp.where(lane == 2 * heads + 2 * h + c, tot[part], stats)
        for h in range(heads):
            part = slice(h * block, (h + 1) * block)
            hv = slice(h * vw, (h + 1) * vw)
            att = dot(jnp.concatenate([p[part] for p in far_p], axis=0), cv_v[:, hv]) + dot(
                jnp.concatenate([p[part] for p in near_p], axis=0), vown[:, hv]
            )
            for c in range(2):
                att_send[h, slots_b, :, c * vw : (c + 1) * vw] = (
                    att[c * block : (c + 1) * block].astype(BF16).reshape(per, rows, vw)
                )
        if block < LANES:
            stats = jnp.concatenate([stats, jnp.zeros((LANES - block, LANES), F32)], axis=0)
        by_row = jnp.transpose(stats)
        group_of = lax.broadcasted_iota(jnp.int32, (most, LANES), 1) // rows
        packed = jnp.zeros((most, LANES), F32)
        for s in range(nstat):
            line = jnp.broadcast_to(by_row[s : s + 1, :], (most, LANES))
            line = pltpu.roll(line, rows, 1, stride=rows, stride_axis=0)
            if s:
                line = pltpu.roll(line, s * rows, 1)
            packed = jnp.where(group_of == s, line, packed)
        for o in range(per):
            st_send[first + o] = packed[most - 1 - o : most - o, :]

    def send_block(peers):
        for peer in peers:
            d = lax.rem(peer - me + kv, kv)

            @pl.when(peer != me)
            def _(peer=peer, d=d):
                to_kv(st_send.at[peer], st_recv.at[d], ss_sem, sr_sem, d).start()

        for peer in peers:
            d = lax.rem(peer - me + kv, kv)

            @pl.when(peer != me)
            def _(peer=peer, d=d):
                for h in range(heads):
                    to_kv(
                        att_send.at[h, peer], att_recv.at[h, d], as_sem, ar_sem, d
                    ).start()

    units = kv // UNIT
    if kv <= UNROLL and kv % (4 * UNIT) == 0:
        quarter, half = kv // 4, kv // 2
        for first, count, peers in (
            (0, quarter, range(quarter)),
            (quarter, half - quarter, range(quarter, half)),
            (half, kv - half, range(half, kv)),
        ):
            for u in range(first // UNIT, (first + count) // UNIT):
                wait_queries(u)
            attend(first, count)
            late = 4 * me >= 3 * kv
            if first == quarter:
                pl.when(lax.rem(mt, 2) == 0)(functools.partial(send_block, range(1, quarter)))
                pl.when(jnp.logical_not(late))(functools.partial(send_block, peers))
            else:
                if first == half:
                    pl.when(late)(functools.partial(send_block, range(quarter, half)))
                    send_block(peers[::2])
                    send_block(peers[1::2])
                else:
                    send_block(peers[:1])
                    pl.when(lax.rem(mt, 2) == 1)(functools.partial(send_block, peers[1:]))
    else:
        for u in range(units):
            wait_queries(u)
        pl.loop(0, blocks)(lambda b: attend(b * per, per))
        send_block(range(kv))
    st_recv[0] = st_send[me]

    for c in small[3:]:
        c.wait()
    hgain = hgain_v[...]
    group = 16
    hrow = lax.broadcasted_iota(jnp.int32, (group, w), 0)
    hcol = lax.broadcasted_iota(jnp.int32, (group, w), 1) // DH
    own_head = hrow == hcol
    row1 = lax.broadcasted_iota(jnp.int32, (group, 1), 0)
    lam_col = jnp.zeros((group, 1), F32)
    for h in range(heads):
        lam_col = jnp.where(row1 == h, lam_s[h], lam_col)
    dk_copy.wait()
    slot_id = lax.broadcasted_iota(jnp.int32, (group, slots), 1)
    vrow = lax.broadcasted_iota(jnp.int32, (group, heads * vw), 0)
    vcol = lax.broadcasted_iota(jnp.int32, (group, heads * vw), 1) // vw
    dec_att = []
    for r in range(drows):
        far_p = []
        near_p = []
        for c in range(2):
            qr = jnp.broadcast_to(dec_q[c][r : r + 1].astype(F32), (group, w))
            qr = jnp.where(own_head, qr, 0.0)
            kr = dec_k[c][r : r + 1].astype(F32)
            near = jnp.sum(qr * kr, axis=-1, keepdims=True)
            far = dot_nt(qr.astype(BF16), dk_v[c, r])
            far = jnp.where(slot_id < len_s[r], far, -jnp.inf)
            top = jnp.maximum(jnp.max(far, axis=-1, keepdims=True), near)
            ef = jnp.exp2((far - top) * C_EXP)
            en = jnp.exp2((near - top) * C_EXP)
            den = jnp.sum(ef, axis=-1, keepdims=True) + en
            far_p.append(ef / den)
            near_p.append(en / den)
        far_w = (far_p[0] - lam_col * far_p[1]).astype(BF16)
        near_w = (near_p[0] - lam_col * near_p[1]).astype(BF16).astype(F32)
        if r == 0:
            dv_copy.wait()
        att = dot(far_w, dv_v[r]) + near_w * dec_v[r : r + 1].astype(F32)
        dec_att.append(jnp.sum(jnp.where(vrow == vcol, att, 0.0), axis=0, keepdims=True))

    def head_norm(att):
        inv = lax.rsqrt(jnp.mean(att * att, axis=-1, keepdims=True) + epsilon)
        return (att * inv * hgain).astype(BF16)

    def to_tp(src, dst, send, recv, d):
        return pltpu.make_async_remote_copy(
            src_ref=src.at[d], dst_ref=dst.at[d], send_sem=send, recv_sem=recv,
            device_id=(me, tp_peer(d)), device_id_type=MESH,
        )

    def out_part(ho, d, h):
        return dot(ho, wo_v[d, h * vw : (h + 1) * vw, :])

    dec_rows = jnp.concatenate(dec_att, axis=0) if drows > 1 else dec_att[0]
    dec_rows = dec_rows if drows > 1 else jnp.broadcast_to(dec_rows, (group, heads * vw))
    dec_ho = [head_norm(dec_rows[:, h * vw : (h + 1) * vw]) for h in range(heads)]
    drain(wo_v, sem_o)
    order = sorted(range(1, tp), key=lambda d: (d < 2, d))

    def dec_project(d):
        acc = None
        for h in range(heads):
            term = out_part(dec_ho[h], d, h)
            acc = term if acc is None else acc + term
        return acc[0:drows].astype(BF16)

    d_sends = {d: to_tp(d_send, d_recv, ds_sem, dr_sem, d) for d in order}
    for d in order:
        d_send[d] = dec_project(d)
        d_sends[d].start()
    dec_own = dec_project(0)

    lane = lax.broadcasted_iota(jnp.int32, (1, LANES), 1)
    p_sends = {d: to_tp(p_send, p_recv, ps_sem, pr_sem, d) for d in order}
    drain(st_recv.at[pl.ds(1, kv - 1)], sr_sem)
    nmax = 2 * heads * rows
    sts = st_recv[...].reshape(kv, LANES)
    top = jnp.max(sts, axis=0, keepdims=True)
    fac = jnp.exp2((sts - top) * C_EXP)
    den = jnp.sum(fac * pltpu.roll(sts, LANES - nmax, 1), axis=0, keepdims=True)
    den = jnp.where(lane < nmax, den, 1.0)
    sign = jnp.ones((1, LANES), F32)
    for h in range(heads):
        sign = jnp.where(lane // rows == 2 * h + 1, -lam_s[h], sign)
    fac = jnp.transpose(fac * (sign / den))
    for i in range(2 * heads):
        for d in range(kv):
            fac_v[i, d] = jnp.broadcast_to(
                fac[i * rows : (i + 1) * rows, d : d + 1], (rows, LANES)
            )
    drain(att_recv.at[:, pl.ds(1, kv - 1)], ar_sem)
    ho = []
    for h in range(heads):
        total_att = None
        for d in range(kv):
            blk = att_send[h, me] if d == 0 else att_recv[h, d]
            for c in range(2):
                f = fac_v[2 * h + c, d]
                term = jnp.concatenate([f] * (vw // LANES), axis=1) * blk[
                    :, c * vw : (c + 1) * vw
                ].astype(F32)
                total_att = term if total_att is None else total_att + term
        ho.append(head_norm(total_att))
    ho = jnp.concatenate(ho, axis=1) if heads > 1 else ho[0]
    for group_d in (order[:1], order[1:] + [0]):
        for d in group_d:
            term = dot(ho, wo_v[d]).astype(BF16)
            if d > 0:
                p_send[d] = term
            else:
                own = term.astype(F32)
        for d in group_d:
            if d > 0:
                p_sends[d].start()
    drain(d_recv.at[pl.ds(1, tp - 1)], dr_sem)
    dsum = dec_own.astype(F32)
    for d in order:
        dsum = dsum + d_recv[d].astype(F32)
    out[rows:, :] = jnp.broadcast_to(dsum, (out.shape[0] - rows, cols)).astype(BF16) if (
        drows == 1
    ) else jnp.concatenate(
        [dsum, jnp.zeros((out.shape[0] - rows - drows, cols), F32)], axis=0
    ).astype(BF16)
    drain(q_all.at[pl.ds(0, kv - 1)], qs_sem)
    drain(st_send.at[pl.ds(0, kv - 1)], ss_sem)
    drain(att_send.at[:, pl.ds(0, kv - 1)], as_sem)
    drain(d_send.at[pl.ds(1, tp - 1)], ds_sem)
    drain(p_send.at[pl.ds(1, tp - 1)], ps_sem)
    drain(p_recv.at[pl.ds(1, tp - 1)], pr_sem)
    for d in order:
        own = own + p_recv[d].astype(F32)
    out[0:rows, :] = own.astype(BF16)


def body(
    tokens, dec_tokens, norm_gain, w_query, w_key, w_value, w_out, head_gain, mix_lambda,
    ctx_keys, ctx_values, dec_keys, dec_values, dec_len, *, kv, tp,
):
    rows, width = tokens.shape
    drows = dec_tokens.shape[0]
    w = w_query.shape[2]
    heads = w // DH
    vwid = w_value.shape[1]
    ctx = ctx_keys.shape[1]
    slots = dec_keys.shape[2]
    cols = w_out.shape[1] // tp
    padded = rows + -(-drows // 16) * 16
    any_spec = pl.BlockSpec(memory_space=pltpu.HBM)
    vmem = pl.BlockSpec(memory_space=pltpu.VMEM)
    dma = pltpu.SemaphoreType.DMA
    V = pltpu.VMEM

    def hbm(x):
        return pltpu.with_memory_space_constraint(x, pltpu.HBM) if x.size > 1 else x

    out = pl.pallas_call(
        functools.partial(kernel, kv, tp),
        out_shape=jax.ShapeDtypeStruct((padded, cols), BF16),
        in_specs=[any_spec] * 8 + [pl.BlockSpec(memory_space=pl.ANY)] * 2 + [any_spec] * 4,
        out_specs=vmem,
        scratch_shapes=[
            pltpu.SMEM((heads,), F32), pltpu.SMEM((drows,), jnp.int32),
            V((rows, width), BF16), V((drows, width), BF16), V((1, width), F32),
            V((1, 2 * DH), F32),
            V((2, width, w), BF16), V((2, width, w), BF16), V((width, vwid), BF16),
            V((tp, vwid, cols), BF16),
            V((2, ctx, w), BF16), V((ctx, vwid), BF16),
            V((2, drows, slots, w), BF16), V((drows, slots, vwid), BF16),
            V((2, w, ctx), BF16), V((2, w, LANES), BF16),
            V((padded, width), BF16), V((kv, rows, 2 * w), BF16),
            V((2, LANES, w), BF16), V((LANES, vwid), BF16),
            V((kv, 1, LANES), F32), V((kv, 1, LANES), F32),
            V((2 * heads, kv, rows, LANES), F32),
            V((heads, kv, rows, 4 * DH), BF16), V((heads, kv, rows, 4 * DH), BF16),
            V((tp, rows, cols), BF16), V((tp, rows, cols), BF16),
            V((tp, drows, cols), BF16), V((tp, drows, cols), BF16),
            dma((6,)), dma((Q_PARTS,)), dma((K_PARTS,)), dma((V_PARTS,)), dma(()),
            dma((2,)), dma((2,)),
            dma(()), dma((kv // UNIT,)), dma(()), dma(()), dma(()), dma(()),
            dma(()), dma(()), dma(()), dma(()),
        ],
        compiler_params=pltpu.CompilerParams(
            collective_id=0, has_side_effects=True, vmem_limit_bytes=48 * 1024 * 1024
        ),
    )(
        hbm(tokens), hbm(dec_tokens), hbm(norm_gain.reshape(1, width)), hbm(w_query),
        hbm(w_key), hbm(w_value), hbm(w_out), hbm(head_gain.reshape(1, 2 * DH)),
        hbm(mix_lambda), hbm(dec_len), hbm(ctx_keys), hbm(ctx_values), hbm(dec_keys),
        hbm(dec_values),
    )

    def split(src, piece_ref, dec_ref):
        piece_ref[...] = src[0:rows, :]
        dec_ref[...] = src[rows : rows + drows, :]

    return pl.pallas_call(
        split,
        out_shape=(
            jax.ShapeDtypeStruct((rows, cols), BF16),
            jax.ShapeDtypeStruct((drows, cols), BF16),
        ),
        in_specs=[vmem],
        out_specs=(vmem, vmem),
        compiler_params=pltpu.CompilerParams(vmem_limit_bytes=1024 * 1024),
    )(out)


def solution(mesh):
    in_specs = (
        P("kv", None),
        P("kv", None),
        P(),
        P(None, None, "tp"),
        P(None, None, "tp"),
        P(None, "tp"),
        P("tp", None),
        P(),
        P("tp"),
        P(None, "kv", "tp"),
        P("kv", "tp"),
        P(None, "kv", None, "tp"),
        P("kv", None, "tp"),
        P("kv"),
    )
    out_specs = (P("kv", "tp"), P("kv", "tp"))
    step = functools.partial(body, kv=mesh.shape["kv"], tp=mesh.shape["tp"])
    return jax.shard_map(step, mesh=mesh, in_specs=in_specs, out_specs=out_specs, check_vma=False)
```

```python
import functools
import math

import jax
import jax.numpy as jnp
from jax import lax
from jax.experimental import pallas as pl
from jax.experimental.pallas import tpu as pltpu
from jax.sharding import PartitionSpec as P

DH = 128
epsilon = 1e-06
MESH = pl.DeviceIdType.MESH
F32 = jnp.float32
BF16 = jnp.bfloat16
LANES = 128
C_EXP = DH ** (-0.5) * math.log2(math.e)
Q_PARTS = 8
K_PARTS = 2
BLOCK = 64
UNROLL = 8
UNIT = 2
V_PARTS = 2


def dot(a, b):
    return jnp.dot(a, b, preferred_element_type=F32)


def dot_nt(a, b):
    return lax.dot_general(a, b, (((1,), (1,)), ((), ())), preferred_element_type=F32)


def piece_block(total):
    return BLOCK if total % BLOCK == 0 else LANES


def kernel(
    kv, tp,
    tokens, dec_tokens, norm_gain, w_query, w_key, w_value, w_out, head_gain,
    mix_lambda, dec_len, ctx_keys, ctx_values, dec_keys, dec_values,
    out,
    lam_s, len_s, tok_v, dtok_v, gain_v, hgain_v, wq_v, wk_v, wv_v, wo_v,
    ck_v, cv_v, dk_v, dv_v,
    kt_v, kn_v, xs, q_all, kown, vown, st_send, st_recv, fac_v, att_send, att_recv, p_send, p_recv,
    d_send, d_recv,
    sem_small, sem_q, sem_k, sem_v, sem_o, sem_c, sem_d,
    qs_sem, qr_sem, ss_sem, sr_sem, as_sem, ar_sem, ps_sem, pr_sem, ds_sem, dr_sem,
):
    me = lax.axis_index("kv")
    mt = lax.axis_index("tp")
    rows, width = tokens.shape
    drows = dec_tokens.shape[0]
    w = w_query.shape[2]
    heads = w // DH
    vw = 2 * DH
    slots = dec_keys.shape[2]
    total = rows * kv
    cols = w_out.shape[1] // tp
    block = piece_block(total)
    blocks = total // block
    padded = xs.shape[0]
    per = block // rows

    def tp_peer(d):
        chip = lax.rem(mt // 2 + d // 2, tp // 2)
        return chip * 2 + lax.rem(mt + d, 2)

    barrier = pltpu.get_barrier_semaphore()
    for d in range(1, kv):
        pl.semaphore_signal(
            barrier, inc=1, device_id=(lax.rem(me + d, kv), mt), device_id_type=MESH
        )
    for d in range(1, tp):
        pl.semaphore_signal(
            barrier, inc=1, device_id=(me, tp_peer(d)), device_id_type=MESH
        )

    small = [
        pltpu.make_async_copy(tokens, tok_v, sem_small.at[0]),
        pltpu.make_async_copy(dec_tokens, dtok_v, sem_small.at[1]),
        pltpu.make_async_copy(norm_gain, gain_v, sem_small.at[2]),
        pltpu.make_async_copy(head_gain, hgain_v, sem_small.at[3]),
        pltpu.make_async_copy(mix_lambda, lam_s, sem_small.at[4]),
        pltpu.make_async_copy(dec_len, len_s, sem_small.at[5]),
    ]
    for c in small:
        c.start()

    qstep = width // Q_PARTS
    kstep = width // K_PARTS
    vstep = width // V_PARTS
    q_copies = []
    for i in range(Q_PARTS):
        sl = (slice(None), pl.ds(i * qstep, qstep))
        q_copies.append(pltpu.make_async_copy(w_query.at[sl], wq_v.at[sl], sem_q.at[i]))
    k_copies = []
    for i in range(K_PARTS):
        sl = (slice(None), pl.ds(i * kstep, kstep))
        k_copies.append(pltpu.make_async_copy(w_key.at[sl], wk_v.at[sl], sem_k.at[i]))
    v_copies = [
        pltpu.make_async_copy(
            w_value.at[pl.ds(i * vstep, vstep)], wv_v.at[pl.ds(i * vstep, vstep)], sem_v.at[i]
        )
        for i in range(V_PARTS)
    ]
    ck_copy = pltpu.make_async_copy(ctx_keys, ck_v, sem_c.at[0])
    cv_copy = pltpu.make_async_copy(ctx_values, cv_v, sem_c.at[1])
    dk_copy = pltpu.make_async_copy(dec_keys, dk_v, sem_d.at[0])
    dv_copy = pltpu.make_async_copy(dec_values, dv_v, sem_d.at[1])
    wo_copies = []
    for d in range(tp):
        start = pl.multiple_of(tp_peer(d) * cols, LANES)
        wo_copies.append(
            pltpu.make_async_copy(w_out.at[:, pl.ds(start, cols)], wo_v.at[d], sem_o)
        )
    for c in q_copies:
        c.start(priority=1)

    kown[...] = jnp.zeros_like(kown)
    vown[...] = jnp.zeros_like(vown)
    xs[rows:, :] = jnp.zeros((padded - rows, width), BF16)
    for c in small[:3]:
        c.wait()
    gain = gain_v[...]

    def normed(x):
        xf = x.astype(F32)
        inv = lax.rsqrt(jnp.mean(xf * xf, axis=-1, keepdims=True) + epsilon)
        return (xf * inv * gain).astype(BF16)

    xs[0:rows, :] = normed(tok_v[...])
    xs[rows : rows + drows, :] = normed(dtok_v[...])

    def to_kv(src, dst, send, recv, d):
        return pltpu.make_async_remote_copy(
            src_ref=src, dst_ref=dst, send_sem=send, recv_sem=recv,
            device_id=(lax.rem(me + d + kv, kv), mt), device_id_type=MESH,
        )

    def drain(ref, sem):
        pltpu.make_async_copy(ref, ref, sem).wait()

    for c in k_copies + [ck_copy]:
        c.start(priority=1)
    acc = [None, None]
    for i in range(Q_PARTS):
        q_copies[i].wait()
        sl = slice(i * qstep, (i + 1) * qstep)
        for c in range(2):
            term = dot(xs[:, sl], wq_v[c, sl, :])
            acc[c] = term if acc[c] is None else acc[c] + term
    dec_q = []
    for c in range(2):
        qc = acc[c].astype(BF16)
        q_all[me, :, c * w : (c + 1) * w] = qc[0:rows]
        dec_q.append(qc[rows:])
    for c in v_copies + [cv_copy]:
        c.start(priority=1)
    pl.semaphore_wait(barrier, kv + tp - 2)
    for i in range(kv - 1):
        ring = sorted(range(1, kv), key=lambda d: (-min(d, kv - d), d))[i]
        half = kv // 2
        if i < half:
            up_first = half + (i ^ 1 if half % 2 == 0 else i) - me
        else:
            near = i - half
            up_first = near + jnp.where(near >= me, 1, 0) - me
        if i < half:
            down_first = half - 1 - i - me
        else:
            down_first = i + jnp.where(i >= me, 1, 0) - me
        d = jnp.where(me < half, up_first, down_first)
        to_kv(q_all.at[me], q_all.at[me], qs_sem, qr_sem.at[lax.div(me, UNIT)], d).start()

    acc = [None, None]
    for i in range(K_PARTS):
        k_copies[i].wait()
        sl = slice(i * kstep, (i + 1) * kstep)
        for c in range(2):
            term = dot(xs[:, sl], wk_v[c, sl, :])
            acc[c] = term if acc[c] is None else acc[c] + term
    dec_k = []
    for c in range(2):
        kc = acc[c].astype(BF16)
        kown[c, 0:rows, :] = kc[0:rows]
        dec_k.append(kc[rows:])
    ck_copy.wait()
    for c in range(2):
        kt_v[c] = jnp.transpose(ck_v[c])
        kn_v[c] = jnp.transpose(kown[c])
    for c in [dk_copy, dv_copy]:
        c.start(priority=1)
    acc = None
    for i in range(V_PARTS):
        v_copies[i].wait()
        term = dot(xs[:, i * vstep : (i + 1) * vstep], wv_v[i * vstep : (i + 1) * vstep, :])
        acc = term if acc is None else acc + term
    vc = acc.astype(BF16)
    vown[0:rows, :] = vc[0:rows]
    dec_v = vc[rows:]
    for c in wo_copies:
        c.start(priority=1)

    cv_copy.wait()
    nstat = 4 * heads
    most = LANES // rows

    def wait_queries(u):
        inside = lax.div(me, UNIT) == u

        @pl.when(inside)
        def _():
            drain(q_all.at[pl.ds(u * UNIT, UNIT - 1)], qr_sem.at[u])

        @pl.when(jnp.logical_not(inside))
        def _():
            drain(q_all.at[pl.ds(u * UNIT, UNIT)], qr_sem.at[u])

    def attend(first, per):
        block = per * rows
        slots_b = pl.ds(first, per)
        qb = q_all[slots_b].reshape(block, 2 * w)
        pos = first * rows + lax.broadcasted_iota(jnp.int32, (block, LANES), 0)
        lane = lax.broadcasted_iota(jnp.int32, (block, LANES), 1)
        ok = (lane < rows) & (lane + me * rows <= pos)
        ok = jnp.concatenate([ok] * heads, axis=0) if heads > 1 else ok
        head_of = lax.broadcasted_iota(jnp.int32, (block, w), 1) // DH
        stats = jnp.zeros((block, LANES), F32)
        far_p = []
        near_p = []
        for c in range(2):
            qc = qb[:, c * w : (c + 1) * w]
            if heads > 1:
                zero = jnp.zeros_like(qc)
                qc = jnp.concatenate(
                    [jnp.where(head_of == h, qc, zero) for h in range(heads)], axis=0
                )
            far = dot(qc, kt_v[c])
            near = dot(qc, kn_v[c])
            near = jnp.where(ok, near, -jnp.inf)
            top = jnp.maximum(
                jnp.max(far, axis=-1, keepdims=True), jnp.max(near, axis=-1, keepdims=True)
            )
            ef = jnp.exp2((far - top) * C_EXP)
            en = jnp.exp2((near - top) * C_EXP)
            tot = jnp.sum(ef, axis=-1, keepdims=True) + jnp.sum(en, axis=-1, keepdims=True)
            far_p.append(ef.astype(BF16))
            near_p.append(en.astype(BF16))
            for h in range(heads):
                part = slice(h * block, (h + 1) * block)
                stats = jnp.where(lane == 2 * h + c, top[part], stats)
                stats = jnp.where(lane == 2 * heads + 2 * h + c, tot[part], stats)
        for h in range(heads):
            part = slice(h * block, (h + 1) * block)
            hv = slice(h * vw, (h + 1) * vw)
            att = dot(jnp.concatenate([p[part] for p in far_p], axis=0), cv_v[:, hv]) + dot(
                jnp.concatenate([p[part] for p in near_p], axis=0), vown[:, hv]
            )
            for c in range(2):
                att_send[h, slots_b, :, c * vw : (c + 1) * vw] = (
                    att[c * block : (c + 1) * block].astype(BF16).reshape(per, rows, vw)
                )
        if block < LANES:
            stats = jnp.concatenate([stats, jnp.zeros((LANES - block, LANES), F32)], axis=0)
        by_row = jnp.transpose(stats)
        group_of = lax.broadcasted_iota(jnp.int32, (most, LANES), 1) // rows
        packed = jnp.zeros((most, LANES), F32)
        for s in range(nstat):
            line = jnp.broadcast_to(by_row[s : s + 1, :], (most, LANES))
            line = pltpu.roll(line, rows, 1, stride=rows, stride_axis=0)
            if s:
                line = pltpu.roll(line, s * rows, 1)
            packed = jnp.where(group_of == s, line, packed)
        for o in range(per):
            st_send[first + o] = packed[most - 1 - o : most - o, :]

    def send_block(peers):
        for peer in peers:
            d = lax.rem(peer - me + kv, kv)

            @pl.when(peer != me)
            def _(peer=peer, d=d):
                to_kv(st_send.at[peer], st_recv.at[d], ss_sem, sr_sem, d).start()

        for peer in peers:
            d = lax.rem(peer - me + kv, kv)

            @pl.when(peer != me)
            def _(peer=peer, d=d):
                for h in range(heads):
                    to_kv(
                        att_send.at[h, peer], att_recv.at[h, d], as_sem, ar_sem, d
                    ).start()

    units = kv // UNIT
    if kv <= UNROLL and kv % (4 * UNIT) == 0:
        quarter, half = kv // 4, kv // 2
        for first, count, peers in (
            (0, quarter, range(quarter)),
            (quarter, half - quarter, range(quarter, half)),
            (half, kv - half, range(half, kv)),
        ):
            for u in range(first // UNIT, (first + count) // UNIT):
                wait_queries(u)
            attend(first, count)
            late = 4 * me >= 3 * kv
            if first == quarter:
                pl.when(lax.rem(mt, 2) == 0)(functools.partial(send_block, range(1, quarter)))
                pl.when(jnp.logical_not(late))(functools.partial(send_block, peers))
            else:
                if first == half:
                    pl.when(late)(functools.partial(send_block, range(quarter, half)))
                    send_block(peers[::2])
                    send_block(peers[1::2])
                else:
                    send_block(peers[:1])
                    pl.when(lax.rem(mt, 2) == 1)(functools.partial(send_block, peers[1:]))
    else:
        for u in range(units):
            wait_queries(u)
        pl.loop(0, blocks)(lambda b: attend(b * per, per))
        send_block(range(kv))
    st_recv[0] = st_send[me]

    for c in small[3:]:
        c.wait()
    hgain = hgain_v[...]
    group = 16
    hrow = lax.broadcasted_iota(jnp.int32, (group, w), 0)
    hcol = lax.broadcasted_iota(jnp.int32, (group, w), 1) // DH
    own_head = hrow == hcol
    row1 = lax.broadcasted_iota(jnp.int32, (group, 1), 0)
    lam_col = jnp.zeros((group, 1), F32)
    for h in range(heads):
        lam_col = jnp.where(row1 == h, lam_s[h], lam_col)
    dk_copy.wait()
    slot_id = lax.broadcasted_iota(jnp.int32, (group, slots), 1)
    vrow = lax.broadcasted_iota(jnp.int32, (group, heads * vw), 0)
    vcol = lax.broadcasted_iota(jnp.int32, (group, heads * vw), 1) // vw
    dec_att = []
    for r in range(drows):
        far_p = []
        near_p = []
        for c in range(2):
            qr = jnp.broadcast_to(dec_q[c][r : r + 1].astype(F32), (group, w))
            qr = jnp.where(own_head, qr, 0.0)
            kr = dec_k[c][r : r + 1].astype(F32)
            near = jnp.sum(qr * kr, axis=-1, keepdims=True)
            far = dot_nt(qr.astype(BF16), dk_v[c, r])
            far = jnp.where(slot_id < len_s[r], far, -jnp.inf)
            top = jnp.maximum(jnp.max(far, axis=-1, keepdims=True), near)
            ef = jnp.exp2((far - top) * C_EXP)
            en = jnp.exp2((near - top) * C_EXP)
            den = jnp.sum(ef, axis=-1, keepdims=True) + en
            far_p.append(ef / den)
            near_p.append(en / den)
        far_w = (far_p[0] - lam_col * far_p[1]).astype(BF16)
        near_w = (near_p[0] - lam_col * near_p[1]).astype(BF16).astype(F32)
        if r == 0:
            dv_copy.wait()
        att = dot(far_w, dv_v[r]) + near_w * dec_v[r : r + 1].astype(F32)
        dec_att.append(jnp.sum(jnp.where(vrow == vcol, att, 0.0), axis=0, keepdims=True))

    def head_norm(att):
        inv = lax.rsqrt(jnp.mean(att * att, axis=-1, keepdims=True) + epsilon)
        return (att * inv * hgain).astype(BF16)

    def to_tp(src, dst, send, recv, d):
        return pltpu.make_async_remote_copy(
            src_ref=src.at[d], dst_ref=dst.at[d], send_sem=send, recv_sem=recv,
            device_id=(me, tp_peer(d)), device_id_type=MESH,
        )

    def out_part(ho, d, h):
        return dot(ho, wo_v[d, h * vw : (h + 1) * vw, :])

    dec_rows = jnp.concatenate(dec_att, axis=0) if drows > 1 else dec_att[0]
    dec_rows = dec_rows if drows > 1 else jnp.broadcast_to(dec_rows, (group, heads * vw))
    dec_ho = [head_norm(dec_rows[:, h * vw : (h + 1) * vw]) for h in range(heads)]
    drain(wo_v, sem_o)
    order = sorted(range(1, tp), key=lambda d: (d < 2, d))

    def dec_project(d):
        acc = None
        for h in range(heads):
            term = out_part(dec_ho[h], d, h)
            acc = term if acc is None else acc + term
        return acc[0:drows].astype(BF16)

    d_sends = {d: to_tp(d_send, d_recv, ds_sem, dr_sem, d) for d in order}
    for d in order:
        d_send[d] = dec_project(d)
        d_sends[d].start()
    dec_own = dec_project(0)

    lane = lax.broadcasted_iota(jnp.int32, (1, LANES), 1)
    p_sends = {d: to_tp(p_send, p_recv, ps_sem, pr_sem, d) for d in order}
    drain(st_recv.at[pl.ds(1, kv - 1)], sr_sem)
    nmax = 2 * heads * rows
    sts = st_recv[...].reshape(kv, LANES)
    top = jnp.max(sts, axis=0, keepdims=True)
    fac = jnp.exp2((sts - top) * C_EXP)
    den = jnp.sum(fac * pltpu.roll(sts, LANES - nmax, 1), axis=0, keepdims=True)
    den = jnp.where(lane < nmax, den, 1.0)
    sign = jnp.ones((1, LANES), F32)
    for h in range(heads):
        sign = jnp.where(lane // rows == 2 * h + 1, -lam_s[h], sign)
    fac = jnp.transpose(fac * (sign / den))
    for i in range(2 * heads):
        for d in range(kv):
            fac_v[i, d] = jnp.broadcast_to(
                fac[i * rows : (i + 1) * rows, d : d + 1], (rows, LANES)
            )
    drain(att_recv.at[:, pl.ds(1, kv - 1)], ar_sem)
    ho = []
    for h in range(heads):
        total_att = None
        for d in range(kv):
            blk = att_send[h, me] if d == 0 else att_recv[h, d]
            for c in range(2):
                f = fac_v[2 * h + c, d]
                term = jnp.concatenate([f] * (vw // LANES), axis=1) * blk[
                    :, c * vw : (c + 1) * vw
                ].astype(F32)
                total_att = term if total_att is None else total_att + term
        ho.append(head_norm(total_att))
    ho = jnp.concatenate(ho, axis=1) if heads > 1 else ho[0]
    for group_d in (order[:1], order[1:] + [0]):
        for d in group_d:
            term = dot(ho, wo_v[d]).astype(BF16)
            if d > 0:
                p_send[d] = term
            else:
                own = term.astype(F32)
        for d in group_d:
            if d > 0:
                p_sends[d].start()
    drain(d_recv.at[pl.ds(1, tp - 1)], dr_sem)
    dsum = dec_own.astype(F32)
    for d in order:
        dsum = dsum + d_recv[d].astype(F32)
    out[rows:, :] = jnp.broadcast_to(dsum, (out.shape[0] - rows, cols)).astype(BF16) if (
        drows == 1
    ) else jnp.concatenate(
        [dsum, jnp.zeros((out.shape[0] - rows - drows, cols), F32)], axis=0
    ).astype(BF16)
    drain(q_all.at[pl.ds(0, kv - 1)], qs_sem)
    drain(st_send.at[pl.ds(0, kv - 1)], ss_sem)
    drain(att_send.at[:, pl.ds(0, kv - 1)], as_sem)
    drain(d_send.at[pl.ds(1, tp - 1)], ds_sem)
    drain(p_send.at[pl.ds(1, tp - 1)], ps_sem)
    drain(p_recv.at[pl.ds(1, tp - 1)], pr_sem)
    for d in order:
        own = own + p_recv[d].astype(F32)
    out[0:rows, :] = own.astype(BF16)


def body(
    tokens, dec_tokens, norm_gain, w_query, w_key, w_value, w_out, head_gain, mix_lambda,
    ctx_keys, ctx_values, dec_keys, dec_values, dec_len, *, kv, tp,
):
    rows, width = tokens.shape
    drows = dec_tokens.shape[0]
    w = w_query.shape[2]
    heads = w // DH
    vwid = w_value.shape[1]
    ctx = ctx_keys.shape[1]
    slots = dec_keys.shape[2]
    cols = w_out.shape[1] // tp
    padded = rows + -(-drows // 16) * 16
    any_spec = pl.BlockSpec(memory_space=pltpu.HBM)
    vmem = pl.BlockSpec(memory_space=pltpu.VMEM)
    dma = pltpu.SemaphoreType.DMA
    V = pltpu.VMEM

    def hbm(x):
        return pltpu.with_memory_space_constraint(x, pltpu.HBM) if x.size > 1 else x

    out = pl.pallas_call(
        functools.partial(kernel, kv, tp),
        out_shape=jax.ShapeDtypeStruct((padded, cols), BF16),
        in_specs=[any_spec] * 8 + [pl.BlockSpec(memory_space=pl.ANY)] * 2 + [any_spec] * 4,
        out_specs=vmem,
        scratch_shapes=[
            pltpu.SMEM((heads,), F32), pltpu.SMEM((drows,), jnp.int32),
            V((rows, width), BF16), V((drows, width), BF16), V((1, width), F32),
            V((1, 2 * DH), F32),
            V((2, width, w), BF16), V((2, width, w), BF16), V((width, vwid), BF16),
            V((tp, vwid, cols), BF16),
            V((2, ctx, w), BF16), V((ctx, vwid), BF16),
            V((2, drows, slots, w), BF16), V((drows, slots, vwid), BF16),
            V((2, w, ctx), BF16), V((2, w, LANES), BF16),
            V((padded, width), BF16), V((kv, rows, 2 * w), BF16),
            V((2, LANES, w), BF16), V((LANES, vwid), BF16),
            V((kv, 1, LANES), F32), V((kv, 1, LANES), F32),
            V((2 * heads, kv, rows, LANES), F32),
            V((heads, kv, rows, 4 * DH), BF16), V((heads, kv, rows, 4 * DH), BF16),
            V((tp, rows, cols), BF16), V((tp, rows, cols), BF16),
            V((tp, drows, cols), BF16), V((tp, drows, cols), BF16),
            dma((6,)), dma((Q_PARTS,)), dma((K_PARTS,)), dma((V_PARTS,)), dma(()),
            dma((2,)), dma((2,)),
            dma(()), dma((kv // UNIT,)), dma(()), dma(()), dma(()), dma(()),
            dma(()), dma(()), dma(()), dma(()),
        ],
        compiler_params=pltpu.CompilerParams(
            collective_id=0, has_side_effects=True, vmem_limit_bytes=48 * 1024 * 1024
        ),
    )(
        hbm(tokens), hbm(dec_tokens), hbm(norm_gain.reshape(1, width)), hbm(w_query),
        hbm(w_key), hbm(w_value), hbm(w_out), hbm(head_gain.reshape(1, 2 * DH)),
        hbm(mix_lambda), hbm(dec_len), hbm(ctx_keys), hbm(ctx_values), hbm(dec_keys),
        hbm(dec_values),
    )

    def split(src, piece_ref, dec_ref):
        piece_ref[...] = src[0:rows, :]
        dec_ref[...] = src[rows : rows + drows, :]

    return pl.pallas_call(
        split,
        out_shape=(
            jax.ShapeDtypeStruct((rows, cols), BF16),
            jax.ShapeDtypeStruct((drows, cols), BF16),
        ),
        in_specs=[vmem],
        out_specs=(vmem, vmem),
        compiler_params=pltpu.CompilerParams(vmem_limit_bytes=1024 * 1024),
    )(out)


def solution(mesh):
    in_specs = (
        P("kv", None),
        P("kv", None),
        P(),
        P(None, None, "tp"),
        P(None, None, "tp"),
        P(None, "tp"),
        P("tp", None),
        P(),
        P("tp"),
        P(None, "kv", "tp"),
        P("kv", "tp"),
        P(None, "kv", None, "tp"),
        P("kv", None, "tp"),
        P("kv"),
    )
    out_specs = (P("kv", "tp"), P("kv", "tp"))
    step = functools.partial(body, kv=mesh.shape["kv"], tp=mesh.shape["tp"])
    return jax.shard_map(step, mesh=mesh, in_specs=in_specs, out_specs=out_specs, check_vma=False)
```
